32 devices in a mesh: ep: 8 (over z, core), tp: 4 (over y, x).
Axes of the slice: x: 2, y: 2, z: 4, core: 2. Of those that a mesh axis runs over, the one named last changes fastest.
Arguments:
- query_rows: bfloat16 [3072, 2048], P('ep', 'tp'), may hold values from -6 to 6
- key_rows: bfloat16 [3072, 2048], P('ep', 'tp'), may hold values from -6 to 6
- value_rows: bfloat16 [3072, 2048], P('ep', 'tp'), may hold values from -6 to 6
- second_scale: float32 [16], P('tp'), may hold values from 0.3 to 0.8
- head_gain: float32 [128], replicated, may hold values from 0.1 to 1.9
- out_weight: bfloat16 [2048, 4096], P(None, 'tp'), may hold values from -0.125 to 0.125
- routed_rows: bfloat16 [1024, 4096], P('ep', 'tp'), may hold values from -6 to 6
- norm_gain: float32 [4096], replicated, may hold values from 0.1 to 1.9
- route_ids: int32 [1024, 2], P('ep'), may hold values from 0 to 7, all different within a row; in each aligned block of 128 rows (0 to 127, 128 to 255, ...) at most 64 rows name the same one
- route_weight: float32 [1024, 2], P('ep'), may hold values from 0.1 to 0.9
- expert_gate: bfloat16 [8, 4096, 2048], P('ep', None, 'tp'), may hold values from -0.09375 to 0.09375
- expert_up: bfloat16 [8, 4096, 2048], P('ep', None, 'tp'), may hold values from -0.09375 to 0.09375
- expert_down: bfloat16 [8, 2048, 4096], P('ep', None, 'tp'), may hold values from -0.125 to 0.125
Outputs:
- mixer_out: bfloat16 [3072, 4096], P('ep', 'tp')
- expert_mix: bfloat16 [1024, 4096], P('ep', 'tp')
The draws below stay inside these ranges and needn't reach their ends.
Inputs may be any that keep to these rules, and one draw needn't show every extreme that they name: `route_ids`: among the 128 tokens of one index of ep, no expert is named by more than 64 of them, a bound that some block reaches.
All inputs are finite; a program needn't handle non-finite values.
Results may differ from the reference program's by a relative error of at most 0.0085.
Values may be sent and summed in bfloat16 or wider, within the bound.
A program may use at most 128 MiB of HBM per device.

```python
import math
import jax
import jax.numpy as jnp
import numpy as np
from jax import lax

D = 4096
HEADS = 16
HD = 64
VD = 128
FF = 2048
TOP = 2
TOK_A = 384
TOK_B = 128
TOKENS_A = 3072
TOKENS_B = 1024
EXPERTS = 8
CAP = 64
N_EP = 8


def draw_query_rows(key, part):
    length_all = TOK_A * N_EP
    drawn_rows = jnp.clip(1.3 * jax.random.normal(jax.random.fold_in(key, 3), (length_all, HEADS * 2 * HD), jnp.float32), -6.0, 6.0)
    return drawn_rows.astype(jnp.bfloat16)


def draw_key_rows(key, part):
    length_all = TOK_A * N_EP
    drawn_rows = jnp.clip(1.3 * jax.random.normal(jax.random.fold_in(key, 5), (length_all, HEADS * 2 * HD), jnp.float32), -6.0, 6.0)
    return drawn_rows.astype(jnp.bfloat16)


def level_of(rng, shape, split, smallest, largest):
    factor_of = 1.0
    for axis_at, parts in split:
        draws = jax.random.uniform(jax.random.fold_in(jax.random.fold_in(rng, 6), axis_at), (parts,), jnp.float32, smallest / len(split), largest / len(split))
        factor_of = factor_of * jnp.repeat(jnp.exp(draws), shape[axis_at] // parts).reshape((-1,) + (1,) * (len(shape) - 1 - axis_at))
    return factor_of


def deal_out(stream_key, own, number, rows, number_of, top, bound, slope):
    order = jax.random.permutation(stream_key, number_of)
    crowded, ordinary = load_shares(number_of, rows * top, bound, slope, True), load_shares(number_of, rows * top, bound, slope, False)
    places = jnp.arange(number_of)

    def named(sizes, offset_by):
        used = int((sizes > 0).sum())
        fixed = max(1, used // 4)
        passed = fixed + (places - fixed + offset_by * (used - fixed)) % max(1, number_of - fixed)
        return jnp.zeros((number_of,), jnp.int32).at[order[jnp.where(places < fixed, places, passed)]].set(jnp.asarray(sizes, jnp.int32))

    sizes = jnp.where(number % 4 == 0, named(crowded, number // 4), named(ordinary, number - number // 4 - 1))
    mixed = jax.random.permutation(jax.random.fold_in(own, 3), number_of)
    giver, sink = mixed[0:number_of // 2 * 2:2], mixed[1:number_of // 2 * 2:2]
    margin = jnp.minimum(sizes[giver] - 1, bound - sizes[sink]) // 2
    margin = jnp.where((giver == order[0]) | (sink == order[0]) | (sizes[sink] == 0), 0, jnp.maximum(margin, 0))
    passed = jax.random.randint(jax.random.fold_in(own, 4), (number_of // 2,), 0, 1 << 20) % (margin + 1)
    sizes = sizes.at[giver].add(-passed).at[sink].add(passed)
    labels = jnp.searchsorted(jnp.cumsum(sizes), jnp.arange(rows * top), side="right").astype(jnp.int32)
    table = labels.reshape(top, rows).T
    table = table[jax.random.permutation(jax.random.fold_in(own, 1), rows)]
    offset_by = jax.random.randint(jax.random.fold_in(own, 2), (rows, 1), 0, top)
    return jnp.take_along_axis(table, (jnp.arange(top)[None, :] + offset_by) % top, axis=1)


def load_shares(amount, total, limit, slope, full):
    loads = [(1 << 20) // math.isqrt(rank ** slope) + 1 for rank in range(1, amount + 1)]
    largest = limit if full else min(limit, max(-(-total // amount), total * loads[0] // sum(loads)))
    least = 1 if total - largest >= amount - 1 else 0
    given, spare = [largest] + [least] * (amount - 1), total - largest - least * (amount - 1)
    while spare > 0:
        free = [i for i in range(1, amount) if given[i] < largest] or [i for i in range(1, amount) if given[i] < limit]
        pool, remaining = sum([loads[i] for i in free]), spare
        for i in free:
            more = min(limit - given[i], max(1, remaining * loads[i] // pool), spare)
            given[i] = given[i] + more
            spare = spare - more
    return np.array(given)


def normal_values(key, dims, spread, reach, pieces=(), held_as=jnp.bfloat16):
    level = level_of(key, dims, pieces, -0.22, 0.18) if pieces else 1.0
    values = jax.random.normal(key, dims, jnp.float32) * spread * level
    return jnp.minimum(jnp.maximum(values, -reach), reach).astype(held_as)


def setup_inputs(seed: int = 0) -> dict:
    keys = jax.random.split(jax.random.key(seed), 14)
    query_rows = draw_query_rows(jax.random.fold_in(keys[13], 71), 0)
    key_rows = draw_key_rows(jax.random.fold_in(keys[13], 71), 0)
    value_rows = normal_values(keys[2], (TOKENS_A, HEADS * VD), 1.0, 6.0, ((0, 8), (1, 4)))
    second_scale = jnp.clip(0.3 + 0.5 * jax.random.uniform(keys[3], (HEADS,), jnp.float32) ** level_of(keys[3], (HEADS,), ((0, 4),), -0.2, 0.2), 0.3, 0.8)
    head_gain = jnp.clip(1.0 + 0.18 * jax.random.normal(keys[4], (VD,), jnp.float32), 0.1, 1.9)
    out_weight = normal_values(keys[5], (HEADS * VD, D), (HEADS * VD) ** -0.5, 0.125, ((1, 4),))
    routed_rows = normal_values(keys[6], (TOKENS_B, D), 1.0, 6.0, ((0, 8), (1, 4)))
    norm_gain = jnp.clip(1.0 + 0.18 * jax.random.normal(keys[7], (D,), jnp.float32), 0.1, 1.9)
    route_ids_keys = jax.random.split(jax.random.fold_in(keys[8], 1), TOKENS_B // TOK_B)
    route_ids_turns = jax.random.permutation(jax.random.fold_in(keys[8], 3), TOKENS_B // TOK_B)
    route_ids = jax.vmap(lambda own, number: deal_out(jax.random.fold_in(keys[8], 2), own, number, TOK_B, EXPERTS, TOP, CAP, 1))(route_ids_keys, route_ids_turns).reshape((TOKENS_B, TOP))
    route_weight = jnp.clip(0.1 + 0.79999997 * jax.random.uniform(keys[9], (TOKENS_B, TOP), jnp.float32) ** level_of(keys[9], (TOKENS_B, TOP), ((0, 8),), -0.2, 0.2), 0.1, 0.9)
    expert_gate = normal_values(keys[10], (EXPERTS, D, FF), D ** -0.5, 0.09375, ((0, 8), (2, 4)))
    expert_up = normal_values(keys[11], (EXPERTS, D, FF), D ** -0.5, 0.09375, ((0, 8), (2, 4)))
    expert_down = normal_values(keys[12], (EXPERTS, FF, D), FF ** -0.5, 0.125, ((0, 8), (2, 4)))
    return {"query_rows": query_rows, "key_rows": key_rows, "value_rows": value_rows, "second_scale": second_scale, "head_gain": head_gain, "out_weight": out_weight, "routed_rows": routed_rows, "norm_gain": norm_gain, "route_ids": route_ids, "route_weight": route_weight, "expert_gate": expert_gate, "expert_up": expert_up, "expert_down": expert_down}


eps = 1e-06
head_factor = 0.8
neg_big = -1e+30

def rms_rows(rows_in, gain):
    floats = rows_in.astype(jnp.float32)
    factor = lax.rsqrt(lax.optimization_barrier(jnp.mean(floats * floats, axis=-1, keepdims=True)) + eps)
    return (floats * factor * gain).astype(jnp.bfloat16)

def reference(query_rows, key_rows, value_rows, second_scale, head_gain, out_weight, routed_rows, norm_gain, route_ids, route_weight, expert_gate, expert_up, expert_down):
    length_all = query_rows.shape[0]
    block_rows = min(512, length_all)
    positions = jnp.arange(length_all, dtype=jnp.int32)
    query_heads = jnp.transpose(query_rows.reshape(length_all, HEADS, 2, HD), (1, 0, 2, 3))
    key_heads = jnp.transpose(key_rows.reshape(length_all, HEADS, 2, HD), (1, 0, 2, 3))
    value_heads = jnp.transpose(value_rows.reshape(length_all, HEADS, VD), (1, 0, 2))

    def one_head(operands):
        query_h, key_h, value_h, scale_h = operands
        key_float = key_h.astype(jnp.float32)
        value_float = value_h.astype(jnp.float32)

        def one_block(block_num):
            row_first = block_num * block_rows
            query_block = lax.dynamic_slice_in_dim(query_h, row_first, block_rows, 0).astype(jnp.float32)
            scores = jnp.einsum('icd,jcd->cij', query_block, key_float) * HD ** (-0.5)
            allowed = ((row_first + jnp.arange(block_rows, dtype=jnp.int32))[:, None] >= positions[None, :])[None]
            scores = jnp.where(allowed, scores, neg_big)
            row_max = lax.optimization_barrier(jnp.max(scores, axis=-1, keepdims=True))
            exp_scores = jnp.where(allowed, jnp.exp(scores - row_max), 0.0)
            denoms = lax.optimization_barrier(jnp.sum(exp_scores, axis=-1))
            rounded = lax.optimization_barrier(exp_scores.astype(jnp.bfloat16)).astype(jnp.float32)
            maps_both = jnp.einsum('cij,je->cie', rounded, value_float) / denoms[..., None]
            mixed_maps = maps_both[0] - scale_h * maps_both[1]
            mean_sq = lax.optimization_barrier(jnp.mean(mixed_maps * mixed_maps, axis=-1, keepdims=True))
            return (mixed_maps * lax.rsqrt(mean_sq + eps) * head_gain * head_factor).astype(jnp.bfloat16)
        block_outs = lax.map(one_block, jnp.arange(length_all // block_rows, dtype=jnp.int32))
        return block_outs.reshape(length_all, VD)
    head_outs = lax.map(one_head, (query_heads, key_heads, value_heads, second_scale))
    head_cat = jnp.transpose(head_outs, (1, 0, 2)).reshape(length_all, HEADS * VD)
    mixer_out = jnp.dot(head_cat, out_weight, preferred_element_type=jnp.float32).astype(jnp.bfloat16)
    normed = rms_rows(routed_rows, norm_gain)
    flat_expert = route_ids.reshape(-1).astype(jnp.int32)
    count_all = flat_expert.shape[0]
    chosen = (flat_expert[:, None] == jnp.arange(EXPERTS, dtype=jnp.int32)[None, :]).astype(jnp.int32)
    ranks = lax.optimization_barrier(jnp.sum((jnp.cumsum(chosen, axis=0) - 1) * chosen, axis=1)).astype(jnp.int32)
    token_of = jnp.arange(count_all, dtype=jnp.int32) // TOP
    table = jnp.full((EXPERTS, N_EP * CAP), TOKENS_B, jnp.int32).at[flat_expert, ranks].set(token_of)
    padded = jnp.concatenate([normed, jnp.zeros((1, D), jnp.bfloat16)], axis=0)

    def one_expert(operands):
        table_row, gate_w, up_w, down_w = operands
        gathered = padded[table_row]
        gate_val = jnp.dot(gathered, gate_w, preferred_element_type=jnp.float32)
        up_val = jnp.dot(gathered, up_w, preferred_element_type=jnp.float32)
        hidden = (jax.nn.silu(gate_val) * up_val).astype(jnp.bfloat16)
        return jnp.dot(hidden, down_w, preferred_element_type=jnp.float32).astype(jnp.bfloat16)
    expert_outs = lax.map(one_expert, (table, expert_gate, expert_up, expert_down))
    picked = expert_outs[flat_expert, ranks].astype(jnp.float32).reshape(TOKENS_B, TOP, D)
    expert_mix = lax.optimization_barrier(jnp.sum(picked * route_weight[:, :, None], axis=1)).astype(jnp.bfloat16)
    return (mixer_out, expert_mix)
```

```python
import functools

import jax
import jax.numpy as jnp
from jax import lax
from jax.experimental import pallas as pl
from jax.experimental.pallas import tpu as pltpu
from jax.sharding import PartitionSpec as P

eps = 1e-06
head_factor = 0.8
neg_big = -1e30
lanes = 2
f32 = jnp.float32
bf16 = jnp.bfloat16


def dot(a, b):
    return jnp.dot(a, b, preferred_element_type=f32)


def layer_kernel(
    n_ep,
    n_tp,
    scale_ref,
    q_hbm,
    k_hbm,
    v_hbm,
    gain_ref,
    wo_hbm,
    rows_hbm,
    norm_ref,
    ids_ref,
    route_w_ref,
    wg_hbm,
    wu_hbm,
    wd_hbm,
    mixer_ref,
    mix_ref,
    q_in,
    q_far,
    q_two,
    k_all,
    v_all,
    rows_all,
    ids_all,
    arr,
    normed,
    hid_all,
    out_e,
    ret,
    head_all,
    spread,
    acc,
    run_max,
    run_sum,
    lse_own,
    lse_far,
    part_out,
    part_in,
    wg,
    wu,
    wd,
    wo,
    local_sem,
    weight_sem,
    rows_up,
    rows_down,
    rows_side,
    rows_recv,
    ids_send,
    ids_recv,
    kv_out,
    kv_side,
    kv_recv,
    far_send,
    far_recv,
    part_send,
    part_recv,
    arr_send,
    arr_recv,
    hid_send,
    hid_recv,
    head_send,
    head_recv,
    ret_send,
    ret_recv,
):
    e = lax.axis_index("ep")
    t = lax.axis_index("tp")
    n_z = n_ep // lanes
    z = lax.div(e, lanes)
    c = lax.rem(e, lanes)
    partner = z * lanes + (1 - c)
    n_tok = q_in.shape[0]
    tok_b = rows_all.shape[1]
    per_head = scale_ref.shape[0]
    head_w = q_two.shape[2]
    val_w = acc.shape[1]
    slots, out_w = ret.shape
    cap = slots // n_ep
    half = n_z // 2
    upper = z >= half
    far = lax.rem(z + half, n_z) * lanes + c
    cols = arr.shape[2]
    hidden_w = hid_all.shape[2]
    route_count = ids_ref.shape[0]

    def remote(src, dst, send, recv, ep_to, tp_to):
        return pltpu.make_async_remote_copy(
            src_ref=src,
            dst_ref=dst,
            send_sem=send,
            recv_sem=recv,
            device_id=(ep_to, tp_to),
            device_id_type=pl.DeviceIdType.MESH,
        )

    def kv_part(ref, j, core):
        return ref.at[j, pl.ds(pl.multiple_of(core * n_tok, n_tok), n_tok)]

    loads = [
        pltpu.make_async_copy(rows_hbm, rows_all.at[e], local_sem.at[0]),
        pltpu.make_async_copy(k_hbm, kv_part(k_all, z, c), local_sem.at[1]),
        pltpu.make_async_copy(v_hbm, kv_part(v_all, z, c), local_sem.at[2]),
        pltpu.make_async_copy(q_hbm, q_in, local_sem.at[3]),
    ]
    for load in loads:
        load.start()
    ids_all[e, pl.ds(0, route_count)] = ids_ref[...]
    weights = [
        pltpu.make_async_copy(wg_hbm.at[0], wg, weight_sem.at[0]),
        pltpu.make_async_copy(wu_hbm.at[0], wu, weight_sem.at[1]),
        pltpu.make_async_copy(wd_hbm.at[0], wd, weight_sem.at[2]),
        pltpu.make_async_copy(wo_hbm, wo, weight_sem.at[3]),
    ]

    barrier = pltpu.get_barrier_semaphore()

    def greet_ep(i, carry):
        to = lax.rem(e + i, n_ep)
        pl.semaphore_signal(barrier, inc=1, device_id=(to, t), device_id_type=pl.DeviceIdType.MESH)
        return carry

    def greet_tp(i, carry):
        to = lax.rem(t + i, n_tp)
        pl.semaphore_signal(barrier, inc=1, device_id=(e, to), device_id_type=pl.DeviceIdType.MESH)
        return carry

    lax.fori_loop(1, n_ep, greet_ep, 0)
    lax.fori_loop(1, n_tp, greet_tp, 0)
    pl.semaphore_wait(barrier, n_ep - 1 + n_tp - 1)
    for load in loads:
        load.wait()

    def ids_copy(to):
        return remote(ids_all.at[e], ids_all.at[e], ids_send.at[to], ids_recv.at[e], to, t)

    def ids_arrival(b):
        return remote(ids_all.at[b], ids_all.at[b], ids_send.at[b], ids_recv.at[b], b, t)

    def rows_copy(block, send, to):
        return remote(rows_all.at[block], rows_all.at[block], send, rows_recv.at[block], to, t)

    def rows_copy_up(j):
        return rows_copy(j * lanes + c, rows_up.at[j], lax.rem(e + lanes, n_ep))

    def rows_copy_down(j):
        return rows_copy(j * lanes + c, rows_down.at[j], lax.rem(e + n_ep - lanes, n_ep))

    def rows_copy_side(j):
        return rows_copy(j * lanes + c, rows_side.at[j], partner)

    def kv_copies(j, core, sems, at, to):
        return [
            remote(
                kv_part(ref, j, core),
                kv_part(ref, j, core),
                sems.at[i, at],
                kv_recv.at[i, j * lanes + core],
                to,
                t,
            )
            for i, ref in enumerate((k_all, v_all))
        ]

    def kv_copies_out(j):
        return kv_copies(z, c, kv_out, j, j * lanes + c)

    def kv_copies_side(j):
        return kv_copies(j, c, kv_side, j, partner)

    def kv_sent_to(j):
        return ((z < half) & (j < half) & (j != z)) | ((z >= half) & (j > z))

    def kv_got_from(j):
        return ((z < half) & (j < half) & (j != z)) | ((j >= half) & (j < z))

    def kv_wait(j, core):
        for copy in kv_copies(j, core, kv_side, j, partner):
            copy.wait_recv()

    def each_z(first, last, cond, work):
        def one(j, carry):
            @pl.when(cond(j))
            def _():
                work(j)

            return carry

        lax.fori_loop(first, last, one, 0)

    def start_all(copies):
        for copy in copies:
            copy.start()

    q_copy = remote(q_in, q_far, far_send.at[0], far_recv.at[0], far, t)
    lse_copy = remote(lse_own, lse_far, far_send.at[1], far_recv.at[1], far, t)

    def part_copy(h):
        return remote(part_out.at[h], part_in.at[h], part_send.at[h], part_recv.at[h], far, t)

    square = n_tp == 4
    across = t + 1 - 2 * lax.rem(t, 2)
    along = lax.rem(t + 2, n_tp)
    corner = n_tp - 1 - t

    def piece(buf, source, i, units):
        step = buf.shape[1] // (2 * units)
        return buf.at[source, pl.ds(i * step, step)]

    def tp_copy(buf, sems, units, source, i, row, to):
        ref = piece(buf, source, i, units)
        return remote(ref, ref, sems[0].at[row, i], sems[1].at[source, i], e, to)

    def tp_peers(work):
        def one(i, carry):
            to = lax.rem(t + i, n_tp)
            work(to, to)
            return carry

        if square:
            work(across, 0)
            work(along, 1)
        else:
            lax.fori_loop(1, n_tp, one, 0)

    def tp_send(buf, sems, units, unit):
        for i in (2 * unit, 2 * unit + 1):
            tp_peers(lambda to, row: tp_copy(buf, sems, units, t, i, row, to).start())

    def tp_hand_on(buf, sems, units, unit):
        if square:
            i = 2 * unit
            tp_copy(buf, sems, units, across, i, 2, across).wait_recv()
            tp_copy(buf, sems, units, across, i, 2, along).start()
            tp_copy(buf, sems, units, along, i + 1, 2, along).wait_recv()
            tp_copy(buf, sems, units, along, i + 1, 2, across).start()

    def tp_arrive(buf, sems, units, unit):
        i = 2 * unit
        if square:
            for source, at in ((across, i + 1), (along, i), (corner, i), (corner, i + 1)):
                tp_copy(buf, sems, units, source, at, 2, source).wait_recv()
        else:
            for at in (i, i + 1):
                tp_peers(lambda to, row: tp_copy(buf, sems, units, to, at, row, to).wait_recv())

    def tp_drain(buf, sems, units):
        for i in range(2 * units):
            tp_peers(lambda to, row: tp_copy(buf, sems, units, t, i, row, to).wait_send())
            if square:
                source, to = (across, along) if i % 2 == 0 else (along, across)
                tp_copy(buf, sems, units, source, i, 2, to).wait_send()

    arr_sems = (arr_send, arr_recv)
    hid_sems = (hid_send, hid_recv)
    head_sems = (head_send, head_recv)

    def unit_of(j):
        return lax.rem(lax.div(j, half) + lax.div(z, half), 2)

    def first_slot(j, side):
        return pl.multiple_of(((unit_of(j) * 2 + side) * half + lax.rem(j, half)) * cap, cap)

    def ret_part(b):
        return ret.at[pl.ds(pl.multiple_of(b * cap, cap), cap)]

    def ret_copy(j, side):
        to = j * lanes + (c if side == 0 else 1 - c)
        return remote(
            out_e.at[pl.ds(first_slot(j, side), cap)],
            ret_part(e),
            ret_send.at[to],
            ret_recv.at[e],
            to,
            t,
        )

    def ret_each(unit, work):
        def one(i, carry):
            j = lax.rem(lax.div(z, half) + unit, 2) * half + i
            if unit == 0:

                @pl.when(j != z)
                def _():
                    work(ret_copy(j, 0))

            else:
                work(ret_copy(j, 0))
            work(ret_copy(j, 1))
            return carry

        lax.fori_loop(0, half, one, 0)

    def ret_arrival(b):
        return remote(ret_part(b), ret_part(b), ret_send.at[b], ret_recv.at[b], b, t)

    def each_ep(work):
        def one(i, carry):
            work(lax.rem(e + i, n_ep))
            return carry

        lax.fori_loop(1, n_ep, one, 0)

    each_ep(lambda to: ids_copy(to).start())

    def pick(block, j, side):
        ids = ids_all[block]
        hit = (ids[0:1] == e).astype(f32)
        for k in range(1, route_count):
            hit = hit + (ids[k : k + 1] == e).astype(f32)
        before = (
            lax.broadcasted_iota(jnp.int32, (tok_b, tok_b), 0)
            < lax.broadcasted_iota(jnp.int32, (tok_b, tok_b), 1)
        ).astype(bf16)
        ranks = dot(jnp.broadcast_to(hit, (16, tok_b)).astype(bf16), before)[0:1]
        slot = lax.broadcasted_iota(jnp.int32, (cap, tok_b), 0).astype(f32)
        chosen = jnp.where((slot == ranks) & (hit > 0.5), 1.0, 0.0).astype(bf16)
        start = first_slot(j, side)
        i = unit_of(j) * 2 + side
        arr[t, pl.ds(start, cap)] = dot(chosen, rows_all[block]).astype(bf16)
        part = arr.at[t, pl.ds(start, cap)]
        tp_peers(
            lambda to, row: remote(
                part, part, arr_send.at[row, i], arr_recv.at[t, i], e, to
            ).start()
        )

    def rows_step(s, carry):
        low, high = z - s, z + s

        @pl.when((s > 0) & (low >= 0))
        def _():
            rows_copy_down(low).wait_recv()

        @pl.when((low >= 0) & (z + 1 < n_z))
        def _():
            rows_copy_up(low).start()

        @pl.when((s > 0) & (high < n_z))
        def _():
            rows_copy_up(high).wait_recv()

        @pl.when((high < n_z) & (z > 0))
        def _():
            rows_copy_down(high).start()

        @pl.when(s == z)
        def _():
            each_z(z + 1, n_z, kv_sent_to, lambda j: start_all(kv_copies_out(j)))
            start_all(kv_copies_side(z))

        @pl.when((s == n_z - 1 - z) & upper)
        def _():
            q_copy.start()

        @pl.when((s == n_z - 1 - z) & (z < half))
        def _():
            each_z(0, z, kv_sent_to, lambda j: start_all(kv_copies_out(j)))

        @pl.when(low >= 0)
        def _():
            rows_copy_side(low).start()

        @pl.when((s > 0) & (high < n_z))
        def _():
            rows_copy_side(high).start()

        def take(j):
            mine, other = j * lanes + c, j * lanes + (1 - c)

            @pl.when(j != z)
            def _():
                ids_arrival(mine).wait_recv()

            pick(mine, j, 0)
            ids_arrival(other).wait_recv()
            rows_copy(other, rows_side.at[j], partner).wait_recv()
            pick(other, j, 1)

        @pl.when(low >= 0)
        def _():
            take(low)

        @pl.when((s > 0) & (high < n_z))
        def _():
            take(high)

        return carry

    lax.fori_loop(0, n_z, rows_step, 0)
    for weight in weights:
        weight.start()
    tp_hand_on(arr, arr_sems, 2, 0)

    lane = lax.broadcasted_iota(jnp.int32, (n_tok, head_w), 1)

    def split_maps(ref, base):
        def one(h, carry):
            scaled = ref[:, pl.ds(pl.multiple_of(h * head_w, head_w), head_w)].astype(f32) * (
                (head_w // 2) ** -0.5
            )
            q_two[base + h, pl.ds(0, n_tok)] = jnp.where(lane < head_w // 2, scaled, 0.0).astype(bf16)
            q_two[base + h, pl.ds(n_tok, n_tok)] = jnp.where(lane < head_w // 2, 0.0, scaled).astype(bf16)
            return carry

        lax.fori_loop(0, per_head, one, 0)

    def attend(base, j, keys_at, n_keys, first, own):
        def one(h, carry):
            slot = base + h
            keys = k_all[j, pl.ds(keys_at, n_keys), pl.ds(pl.multiple_of(h * head_w, head_w), head_w)]
            values = v_all[j, pl.ds(keys_at, n_keys), pl.ds(pl.multiple_of(h * val_w, val_w), val_w)].T

            def score(m):
                scores = lax.dot_general(
                    keys,
                    q_two[slot, pl.ds(m * n_tok, n_tok)],
                    (((1,), (1,)), ((), ())),
                    preferred_element_type=f32,
                )
                if own:
                    scores = jnp.where(
                        lax.broadcasted_iota(jnp.int32, (n_keys, n_tok), 0)
                        <= lax.broadcasted_iota(jnp.int32, (n_keys, n_tok), 1),
                        scores,
                        neg_big,
                    )
                return scores

            both = [score(m) for m in range(2)]
            for m in range(2):
                part = pl.ds(m * n_tok, n_tok)
                scores = both[m]
                top = jnp.max(scores, axis=0, keepdims=True)
                if not first:
                    old = run_max[slot, :, part]
                    top = jnp.maximum(old, top)
                shares = jnp.exp(scores - top)
                total = jnp.sum(shares, axis=0, keepdims=True)
                update = dot(values, shares.astype(bf16))
                if not first:
                    shrink = jnp.exp(old - top)
                    total = total + run_sum[slot, :, part] * shrink
                    update = update + acc[slot, :, part] * shrink
                run_max[slot, :, part] = top
                run_sum[slot, :, part] = total
                acc[slot, :, part] = update
            return carry

        lax.fori_loop(0, per_head, one, 0)

    def attend_chip(base, j, first):
        attend(base, j, 0, lanes * n_tok, first, False)

    def core_at(core):
        return pl.multiple_of(core * n_tok, n_tok)

    split_maps(q_in, 0)
    attend(0, z, core_at(c), n_tok, True, True)
    kv_wait(z, 1 - c)

    @pl.when(c == 1)
    def _():
        attend(0, z, core_at(1 - c), n_tok, False, False)

    tp_hand_on(arr, arr_sems, 2, 1)

    def kv_arrive(j):
        kv_wait(j, c)
        start_all(kv_copies_side(j))

    def put_lse(base):
        for h in range(per_head):
            total = run_max[base + h] + jnp.log(run_sum[base + h])
            for m in range(2):
                lse_own[2 * h + m : 2 * h + m + 1] = total[:, m * n_tok : (m + 1) * n_tok]

    def mixed_maps(base, h, shared):
        maps = []
        for m in range(2):
            part = pl.ds(m * n_tok, n_tok)
            weight = 1.0 / run_sum[base + h, :, part]
            if shared:
                row = pl.ds(2 * h + m, 1)
                weight = weight / (1.0 + jnp.exp(lse_far[row] - lse_own[row]))
            maps.append((acc[base + h, :, part], weight))
        (first, first_w), (second, second_w) = maps
        return first * first_w - second * (second_w * scale_ref[h])

    for weight in weights:
        weight.wait()
    unit_rows = slots // 2
    n_rows = min(unit_rows, 64)
    tile_f = min(hidden_w, 256)

    def expert_in(unit):
        tp_arrive(arr, arr_sems, 2, unit)

        def norm_step(i, carry):
            part = pl.ds(pl.multiple_of(unit * unit_rows + i * n_rows, n_rows), n_rows)
            squares = jnp.zeros((n_rows, 1), f32)
            for p in range(n_tp):
                x = arr[p, part].astype(f32)
                squares = squares + jnp.sum(x * x, axis=-1, keepdims=True)
            factor = lax.rsqrt(squares / (n_tp * cols) + eps)
            for p in range(n_tp):
                where = pl.ds(p * cols, cols)
                normed[part, where] = (
                    arr[p, part].astype(f32) * factor * norm_ref[0:1, where]
                ).astype(bf16)
            return carry

        lax.fori_loop(0, unit_rows // n_rows, norm_step, 0)
        rows = pl.ds(unit * unit_rows, unit_rows)

        def gate_step(i, carry):
            where = pl.ds(pl.multiple_of(i * tile_f, tile_f), tile_f)
            gate = dot(normed[rows], wg[:, where])
            up = dot(normed[rows], wu[:, where])
            hid_all[t, rows, where] = (gate / (1.0 + jnp.exp(-gate)) * up).astype(bf16)
            return carry

        lax.fori_loop(0, hidden_w // tile_f, gate_step, 0)
        tp_send(hid_all, hid_sems, 2, unit)

    expert_in(0)

    @pl.when(z < half)
    def _():
        q_copy.wait_recv()
        split_maps(q_far, per_head)
        attend_chip(per_head, z, True)

    each_z(0, n_z, kv_got_from, kv_arrive)

    @pl.when(z < half)
    def _():
        def one(j):
            kv_wait(j, 1 - c)
            attend_chip(per_head, j, False)

        each_z(0, half, kv_got_from, one)
        put_lse(per_head)
        lse_copy.start()

    @pl.when(upper)
    def _():
        def one(j):
            kv_wait(j, 1 - c)
            attend_chip(0, j, False)

        each_z(half, n_z, kv_got_from, one)
        put_lse(0)
        lse_copy.start()

    expert_in(1)

    @pl.when(z < half)
    def _():
        lse_copy.wait_recv()
        for h in range(per_head):
            part_out[h] = mixed_maps(per_head, h, True).astype(bf16)
            part_copy(h).start()
        each_z(0, z, kv_got_from, lambda j: attend_chip(0, j, False))

    tp_hand_on(hid_all, hid_sems, 2, 0)
    tp_hand_on(hid_all, hid_sems, 2, 1)
    tile_o = min(out_w, 256)

    def expert_out(unit):
        tp_arrive(hid_all, hid_sems, 2, unit)
        rows = pl.ds(unit * unit_rows, unit_rows)

        def down_step(i, carry):
            where = pl.ds(pl.multiple_of(i * tile_o, tile_o), tile_o)
            total = dot(hid_all[0, rows], wd[pl.ds(0, hidden_w), where])
            for p in range(1, n_tp):
                total = total + dot(hid_all[p, rows], wd[pl.ds(p * hidden_w, hidden_w), where])
            out_e[rows, where] = total.astype(bf16)
            return carry

        lax.fori_loop(0, out_w // tile_o, down_step, 0)
        ret_each(unit, lambda copy: copy.start())

    expert_out(0)
    expert_out(1)
    ret[pl.ds(pl.multiple_of(e * cap, cap), cap)] = out_e[pl.ds(first_slot(z, 0), cap)]

    def head_step(h, mixed):
        mean_sq = jnp.mean(mixed * mixed, axis=0, keepdims=True)
        normal = mixed * lax.rsqrt(mean_sq + eps) * gain_ref[...] * head_factor
        head_all[t, :, h * val_w : (h + 1) * val_w] = normal.T.astype(bf16)

    @pl.when(z < half)
    def _():
        for h in range(per_head):
            head_step(h, mixed_maps(0, h, False))

    @pl.when(upper)
    def _():
        lse_copy.wait_recv()
        for h in range(per_head):
            part_copy(h).wait_recv()
            head_step(h, mixed_maps(0, h, True) + part_in[h].astype(f32))

    tp_send(head_all, head_sems, 1, 0)

    row_of = lax.broadcasted_iota(jnp.int32, (tok_b, tok_b), 0)
    col_of = lax.broadcasted_iota(jnp.int32, (tok_b, tok_b), 1)

    def column(row):
        return jnp.sum(
            jnp.where(row_of == col_of, row.astype(f32), 0.0), axis=1, keepdims=True
        )

    shares = []
    for k in range(route_count):
        ids = column(ids_ref[k : k + 1])
        same = jnp.zeros((tok_b, tok_b), f32)
        for other in range(route_count):
            same = same + (ids_ref[other : other + 1].astype(f32) == ids).astype(f32)
        ranks = jnp.sum(jnp.where(col_of < row_of, same, 0.0), axis=1, keepdims=True)
        slot = lax.broadcasted_iota(jnp.int32, (tok_b, slots), 1).astype(f32)
        spread[k] = jnp.where(slot == ids * cap + ranks, 1.0, 0.0).astype(bf16)
        shares.append(column(route_w_ref[k : k + 1]))

    tp_hand_on(head_all, head_sems, 1, 0)
    tp_arrive(head_all, head_sems, 1, 0)
    heads_w = head_all.shape[2]

    def mixer_step(i, carry):
        where = pl.ds(pl.multiple_of(i * tile_o, tile_o), tile_o)
        total = dot(head_all[0], wo[pl.ds(0, heads_w), where])
        for p in range(1, n_tp):
            total = total + dot(head_all[p], wo[pl.ds(p * heads_w, heads_w), where])
        mixer_ref[:, where] = total.astype(bf16)
        return carry

    lax.fori_loop(0, out_w // tile_o, mixer_step, 0)

    each_ep(lambda b: ret_arrival(b).wait_recv())
    tile_m = min(out_w, 256)
    for start in range(0, out_w, tile_m):
        where = pl.ds(start, tile_m)
        total = shares[0] * dot(spread[0], ret[:, where])
        for k in range(1, route_count):
            total = total + shares[k] * dot(spread[k], ret[:, where])
        mix_ref[:, where] = total.astype(bf16)

    each_ep(lambda to: ids_copy(to).wait_send())
    for unit in range(2):
        ret_each(unit, lambda copy: copy.wait_send())
    tp_drain(arr, arr_sems, 2)
    tp_drain(hid_all, hid_sems, 2)
    tp_drain(head_all, head_sems, 1)

    def drain(j, carry):
        rows_copy_side(j).wait_send()

        @pl.when((j <= z) & (z + 1 < n_z))
        def _():
            rows_copy_up(j).wait_send()

        @pl.when((j >= z) & (z > 0))
        def _():
            rows_copy_down(j).wait_send()

        @pl.when(kv_sent_to(j))
        def _():
            for copy in kv_copies_out(j):
                copy.wait_send()

        @pl.when((j == z) | kv_got_from(j))
        def _():
            for copy in kv_copies_side(j):
                copy.wait_send()

        return carry

    lax.fori_loop(0, n_z, drain, 0)
    lse_copy.wait_send()

    @pl.when(upper)
    def _():
        q_copy.wait_send()

    @pl.when(z < half)
    def _():
        for h in range(per_head):
            part_copy(h).wait_send()


def per_device(
    n_ep,
    n_tp,
    query_rows,
    key_rows,
    value_rows,
    second_scale,
    head_gain,
    out_weight,
    routed_rows,
    norm_gain,
    route_ids,
    route_weight,
    expert_gate,
    expert_up,
    expert_down,
):
    n_tok, attn_w = query_rows.shape
    per_head = second_scale.shape[0]
    val_w = head_gain.shape[0]
    head_w = attn_w // per_head
    tok_b, cols = routed_rows.shape
    route_count = route_ids.shape[1]
    hidden_w = expert_gate.shape[2]
    out_w = out_weight.shape[1]
    n_z = n_ep // lanes
    cap = 2 * tok_b * route_count // n_ep
    slots = n_ep * cap
    vmem = pl.BlockSpec(memory_space=pltpu.VMEM)
    hbm = pl.BlockSpec(memory_space=pl.ANY)
    dma = pltpu.SemaphoreType.DMA
    return pl.pallas_call(
        functools.partial(layer_kernel, n_ep, n_tp),
        out_shape=(
            jax.ShapeDtypeStruct((n_tok, out_w), bf16),
            jax.ShapeDtypeStruct((tok_b, out_w), bf16),
        ),
        in_specs=[
            pl.BlockSpec(memory_space=pltpu.SMEM),
            hbm,
            hbm,
            hbm,
            vmem,
            hbm,
            hbm,
            vmem,
            vmem,
            vmem,
            hbm,
            hbm,
            hbm,
        ],
        out_specs=(vmem, vmem),
        scratch_shapes=[
            pltpu.VMEM((n_tok, attn_w), bf16),
            pltpu.VMEM((n_tok, attn_w), bf16),
            pltpu.VMEM((2 * per_head, 2 * n_tok, head_w), bf16),
            pltpu.VMEM((n_z, lanes * n_tok, attn_w), bf16),
            pltpu.VMEM((n_z, lanes * n_tok, value_rows.shape[1]), bf16),
            pltpu.VMEM((n_ep, tok_b, cols), bf16),
            pltpu.VMEM((n_ep, 8, tok_b), jnp.int32),
            pltpu.VMEM((n_tp, slots, cols), bf16),
            pltpu.VMEM((slots, n_tp * cols), bf16),
            pltpu.VMEM((n_tp, slots, hidden_w), bf16),
            pltpu.VMEM((slots, out_w), bf16),
            pltpu.VMEM((slots, out_w), bf16),
            pltpu.VMEM((n_tp, n_tok, per_head * val_w), bf16),
            pltpu.VMEM((route_count, tok_b, slots), bf16),
            pltpu.VMEM((2 * per_head, val_w, 2 * n_tok), f32),
            pltpu.VMEM((2 * per_head, 1, 2 * n_tok), f32),
            pltpu.VMEM((2 * per_head, 1, 2 * n_tok), f32),
            pltpu.VMEM((2 * per_head, n_tok), f32),
            pltpu.VMEM((2 * per_head, n_tok), f32),
            pltpu.VMEM((per_head, val_w, n_tok), bf16),
            pltpu.VMEM((per_head, val_w, n_tok), bf16),
            pltpu.VMEM(expert_gate.shape[1:], bf16),
            pltpu.VMEM(expert_up.shape[1:], bf16),
            pltpu.VMEM(expert_down.shape[1:], bf16),
            pltpu.VMEM(out_weight.shape, bf16),
            dma((4,)),
            dma((4,)),
            dma((n_z,)),
            dma((n_z,)),
            dma((n_z,)),
            dma((n_ep,)),
            dma((n_ep,)),
            dma((n_ep,)),
            dma((2, n_z)),
            dma((2, n_z)),
            dma((2, n_ep)),
            dma((2,)),
            dma((2,)),
            dma((per_head,)),
            dma((per_head,)),
            dma((n_tp, 4)),
            dma((n_tp, 4)),
            dma((n_tp, 4)),
            dma((n_tp, 4)),
            dma((n_tp, 2)),
            dma((n_tp, 2)),
            dma((n_ep,)),
            dma((n_ep,)),
        ],
        compiler_params=pltpu.CompilerParams(
            collective_id=0, has_side_effects=True, vmem_limit_bytes=66000000
        ),
    )(
        second_scale,
        query_rows,
        key_rows,
        value_rows,
        head_gain.reshape(-1, 1),
        out_weight,
        routed_rows,
        norm_gain.reshape(1, -1),
        route_ids.T,
        route_weight.T,
        expert_gate,
        expert_up,
        expert_down,
    )


def solution(mesh):
    placed = (
        P("ep", "tp"),
        P("ep", "tp"),
        P("ep", "tp"),
        P("tp"),
        P(),
        P(None, "tp"),
        P("ep", "tp"),
        P(),
        P("ep", None),
        P("ep", None),
        P("ep", None, "tp"),
        P("ep", None, "tp"),
        P("ep", None, "tp"),
    )
    return jax.shard_map(
        functools.partial(per_device, mesh.shape["ep"], mesh.shape["tp"]),
        mesh=mesh,
        in_specs=placed,
        out_specs=(P("ep", "tp"), P("ep", "tp")),
        check_vma=False,
    )
```

```python
import functools

import jax
import jax.numpy as jnp
from jax import lax
from jax.experimental import pallas as pl
from jax.experimental.pallas import tpu as pltpu
from jax.sharding import PartitionSpec as P

eps = 1e-06
head_factor = 0.8
neg_big = -1e30
lanes = 2
f32 = jnp.float32
bf16 = jnp.bfloat16


def dot(a, b):
    return jnp.dot(a, b, preferred_element_type=f32)


def layer_kernel(
    n_ep,
    n_tp,
    scale_ref,
    q_hbm,
    k_hbm,
    v_hbm,
    gain_ref,
    wo_hbm,
    rows_hbm,
    norm_ref,
    ids_ref,
    route_w_ref,
    wg_hbm,
    wu_hbm,
    wd_hbm,
    mixer_ref,
    mix_ref,
    q_in,
    q_far,
    q_two,
    k_all,
    v_all,
    rows_all,
    ids_all,
    arr,
    normed,
    hid_all,
    out_e,
    ret,
    head_all,
    spread,
    acc,
    run_max,
    run_sum,
    lse_own,
    lse_far,
    part_out,
    part_in,
    wg,
    wu,
    wd,
    wo,
    local_sem,
    weight_sem,
    rows_up,
    rows_down,
    rows_side,
    rows_recv,
    ids_send,
    ids_recv,
    kv_out,
    kv_side,
    kv_recv,
    far_send,
    far_recv,
    lse_send,
    lse_recv,
    part_send,
    part_recv,
    arr_send,
    arr_recv,
    hid_send,
    hid_recv,
    head_send,
    head_recv,
    ret_send,
    ret_recv,
):
    e = lax.axis_index("ep")
    t = lax.axis_index("tp")
    n_z = n_ep // lanes
    z = lax.div(e, lanes)
    c = lax.rem(e, lanes)
    partner = z * lanes + (1 - c)
    n_tok = q_in.shape[0]
    tok_b = rows_all.shape[1]
    per_head = scale_ref.shape[0]
    head_w = q_two.shape[2]
    val_w = acc.shape[1]
    slots, out_w = ret.shape
    cap = slots // n_ep
    half = n_z // 2
    upper = z >= n_z - 2
    worker = (z >= n_z - 4) & (z < n_z - 2)
    far = jnp.where(upper, z - 2, lax.rem(z + 2, n_z)) * lanes + c
    cols = arr.shape[2]
    hidden_w = hid_all.shape[2]
    route_count = ids_ref.shape[0]

    def remote(src, dst, send, recv, ep_to, tp_to):
        return pltpu.make_async_remote_copy(
            src_ref=src,
            dst_ref=dst,
            send_sem=send,
            recv_sem=recv,
            device_id=(ep_to, tp_to),
            device_id_type=pl.DeviceIdType.MESH,
        )

    def kv_part(ref, j, core):
        return ref.at[j, pl.ds(pl.multiple_of(core * n_tok, n_tok), n_tok)]

    loads = [
        pltpu.make_async_copy(rows_hbm, rows_all.at[e], local_sem.at[0]),
        pltpu.make_async_copy(k_hbm, kv_part(k_all, z, c), local_sem.at[1]),
        pltpu.make_async_copy(v_hbm, kv_part(v_all, z, c), local_sem.at[2]),
        pltpu.make_async_copy(q_hbm, q_in, local_sem.at[3]),
    ]
    for load in loads:
        load.start()
    ids_all[e, pl.ds(0, route_count)] = ids_ref[...]
    weights = [
        pltpu.make_async_copy(wg_hbm.at[0], wg, weight_sem.at[0]),
        pltpu.make_async_copy(wu_hbm.at[0], wu, weight_sem.at[1]),
        pltpu.make_async_copy(wd_hbm.at[0], wd, weight_sem.at[2]),
        pltpu.make_async_copy(wo_hbm, wo, weight_sem.at[3]),
    ]

    barrier = pltpu.get_barrier_semaphore()

    def greet_ep(i, carry):
        to = lax.rem(e + i, n_ep)
        pl.semaphore_signal(barrier, inc=1, device_id=(to, t), device_id_type=pl.DeviceIdType.MESH)
        return carry

    def greet_tp(i, carry):
        to = lax.rem(t + i, n_tp)
        pl.semaphore_signal(barrier, inc=1, device_id=(e, to), device_id_type=pl.DeviceIdType.MESH)
        return carry

    lax.fori_loop(1, n_ep, greet_ep, 0)
    lax.fori_loop(1, n_tp, greet_tp, 0)
    with jax.named_scope("barrier"):
        pl.semaphore_wait(barrier, n_ep - 1 + n_tp - 1)
        for load in loads:
            load.wait()

    def ids_copy(to):
        return remote(ids_all.at[e], ids_all.at[e], ids_send.at[to], ids_recv.at[e], to, t)

    def ids_arrival(b):
        return remote(ids_all.at[b], ids_all.at[b], ids_send.at[b], ids_recv.at[b], b, t)

    def rows_copy(block, send, to):
        return remote(rows_all.at[block], rows_all.at[block], send, rows_recv.at[block], to, t)

    def rows_copy_up(j):
        return rows_copy(j * lanes + c, rows_up.at[j], lax.rem(e + lanes, n_ep))

    def rows_copy_down(j):
        return rows_copy(j * lanes + c, rows_down.at[j], lax.rem(e + n_ep - lanes, n_ep))

    def rows_copy_side(j):
        return rows_copy(j * lanes + c, rows_side.at[j], partner)

    def kv_copies(j, core, sems, at, to):
        return [
            remote(
                kv_part(ref, j, core),
                kv_part(ref, j, core),
                sems.at[i, at],
                kv_recv.at[i, j * lanes + core],
                to,
                t,
            )
            for i, ref in enumerate((k_all, v_all))
        ]

    def kv_copies_out(j):
        return kv_copies(z, c, kv_out, j, j * lanes + c)

    def kv_copies_side(j):
        return kv_copies(j, c, kv_side, j, partner)

    def kv_sent_to(j):
        return (j > z) & ((j < n_z - 2) | (j == z + 1))

    def kv_got_from(j):
        return (j < z) & ((z < n_z - 2) | (j == z - 1))

    def kv_wait(j, core):
        for copy in kv_copies(j, core, kv_side, j, partner):
            copy.wait_recv()

    def each_z(first, last, cond, work):
        def one(j, carry):
            @pl.when(cond(j))
            def _():
                work(j)

            return carry

        lax.fori_loop(first, last, one, 0)

    def start_all(copies):
        for copy in copies:
            copy.start()

    q_copy = remote(q_in, q_far, far_send, far_recv, far, t)

    def lse_copy(h):
        return remote(lse_own.at[h], lse_far.at[h], lse_send.at[h], lse_recv.at[h], far, t)

    def part_copy(h):
        return remote(part_out.at[h], part_in.at[h], part_send.at[h], part_recv.at[h], far, t)

    square = n_tp == 4
    across = t + 1 - 2 * lax.rem(t, 2)
    along = lax.rem(t + 2, n_tp)
    corner = n_tp - 1 - t

    def piece(buf, source, i, units):
        if buf is head_all:
            step = n_tok // 2
            cols_at = pl.ds((i // 2) * val_w, val_w)
            return buf.at[source, pl.ds((i % 2) * step, step), cols_at]
        step = buf.shape[1] // (2 * units)
        return buf.at[source, pl.ds(i * step, step)]

    def tp_copy(buf, sems, units, source, i, row, to):
        ref = piece(buf, source, i, units)
        return remote(ref, ref, sems[0].at[row, i], sems[1].at[source, i], e, to)

    def tp_peers(work):
        def one(i, carry):
            to = lax.rem(t + i, n_tp)
            work(to, to)
            return carry

        if square:
            work(across, 0)
            work(along, 1)
        else:
            lax.fori_loop(1, n_tp, one, 0)

    def tp_send(buf, sems, units, unit):
        for i in (2 * unit, 2 * unit + 1):
            tp_peers(lambda to, row: tp_copy(buf, sems, units, t, i, row, to).start())

    def tp_hand_on(buf, sems, units, unit):
        if square:
            i = 2 * unit
            tp_copy(buf, sems, units, across, i, 2, across).wait_recv()
            tp_copy(buf, sems, units, across, i, 2, along).start()
            tp_copy(buf, sems, units, along, i + 1, 2, along).wait_recv()
            tp_copy(buf, sems, units, along, i + 1, 2, across).start()

    def tp_arrive(buf, sems, units, unit):
        i = 2 * unit
        if square:
            for source, at in ((across, i + 1), (along, i), (corner, i), (corner, i + 1)):
                tp_copy(buf, sems, units, source, at, 2, source).wait_recv()
        else:
            for at in (i, i + 1):
                tp_peers(lambda to, row: tp_copy(buf, sems, units, to, at, row, to).wait_recv())

    def tp_drain(buf, sems, units):
        for i in range(2 * units):
            tp_peers(lambda to, row: tp_copy(buf, sems, units, t, i, row, to).wait_send())
            if square:
                source, to = (across, along) if i % 2 == 0 else (along, across)
                tp_copy(buf, sems, units, source, i, 2, to).wait_send()

    arr_sems = (arr_send, arr_recv)
    hid_sems = (hid_send, hid_recv)
    head_sems = (head_send, head_recv)

    def unit_of(j):
        return lax.rem(lax.div(j, half) + lax.div(z, half), 2)

    def first_slot(j, side):
        return pl.multiple_of(((unit_of(j) * 2 + side) * half + lax.rem(j, half)) * cap, cap)

    def ret_part(b):
        return ret.at[pl.ds(pl.multiple_of(b * cap, cap), cap)]

    def ret_copy(j, side):
        to = j * lanes + (c if side == 0 else 1 - c)
        return remote(
            out_e.at[pl.ds(first_slot(j, side), cap)],
            ret_part(e),
            ret_send.at[to],
            ret_recv.at[e],
            to,
            t,
        )

    def ret_each(unit, work):
        def one(i, carry):
            j = lax.rem(lax.div(z, half) + unit, 2) * half + i
            if unit == 0:

                @pl.when(j != z)
                def _():
                    work(ret_copy(j, 0))

            else:
                work(ret_copy(j, 0))
            work(ret_copy(j, 1))
            return carry

        lax.fori_loop(0, half, one, 0)

    def ret_arrival(b):
        return remote(ret_part(b), ret_part(b), ret_send.at[b], ret_recv.at[b], b, t)

    def each_ep(work):
        def one(i, carry):
            work(lax.rem(e + i, n_ep))
            return carry

        lax.fori_loop(1, n_ep, one, 0)

    each_ep(lambda to: ids_copy(to).start())

    def pick(block, j, side):
        ids = ids_all[block]
        hit = (ids[0:1] == e).astype(f32)
        for k in range(1, route_count):
            hit = hit + (ids[k : k + 1] == e).astype(f32)
        before = (
            lax.broadcasted_iota(jnp.int32, (tok_b, tok_b), 0)
            < lax.broadcasted_iota(jnp.int32, (tok_b, tok_b), 1)
        ).astype(bf16)
        ranks = dot(jnp.broadcast_to(hit, (16, tok_b)).astype(bf16), before)[0:1]
        slot = lax.broadcasted_iota(jnp.int32, (cap, tok_b), 0).astype(f32)
        chosen = jnp.where((slot == ranks) & (hit > 0.5), 1.0, 0.0).astype(bf16)
        start = first_slot(j, side)
        i = unit_of(j) * 2 + side
        arr[t, pl.ds(start, cap)] = dot(chosen, rows_all[block]).astype(bf16)
        part = arr.at[t, pl.ds(start, cap)]
        tp_peers(
            lambda to, row: remote(
                part, part, arr_send.at[row, i], arr_recv.at[t, i], e, to
            ).start()
        )

    def rows_left_up(j, carry):
        rows_copy_up(j).wait_send()
        return carry

    def rows_left_down(j, carry):
        rows_copy_down(j).wait_send()
        return carry

    def rows_step(s, carry):
        low, high = z - s, z + s

        @pl.when((s > 0) & (low >= 0))
        def _():
            rows_copy_down(low).wait_recv()

        @pl.when((low >= 0) & (z + 1 < n_z))
        def _():
            rows_copy_up(low).start()

        @pl.when((s > 0) & (high < n_z))
        def _():
            rows_copy_up(high).wait_recv()

        @pl.when((high < n_z) & (z > 0))
        def _():
            rows_copy_down(high).start()

        @pl.when(s == 1)
        def _():
            start_all(kv_copies_side(z))
            for weight in weights:
                weight.start()

        @pl.when(s == z + 1)
        def _():
            lax.fori_loop(0, s, rows_left_up, 0)
            each_z(s, n_z, kv_sent_to, lambda j: start_all(kv_copies_out(j)))

        @pl.when(low >= 0)
        def _():
            rows_copy_side(low).start()

        @pl.when((s > 0) & (high < n_z))
        def _():
            rows_copy_side(high).start()

        @pl.when(s == half)
        def _():
            @pl.when(upper)
            def _():
                lax.fori_loop(z, n_z, rows_left_down, 0)
                q_copy.start()

            with jax.named_scope("arr_hand0"):
                tp_hand_on(arr, arr_sems, 2, 0)

        def take(j):
            mine, other = j * lanes + c, j * lanes + (1 - c)

            @pl.when(j != z)
            def _():
                ids_arrival(mine).wait_recv()

            pick(mine, j, 0)
            ids_arrival(other).wait_recv()
            rows_copy(other, rows_side.at[j], partner).wait_recv()
            pick(other, j, 1)

        up_first = z >= half

        @pl.when(up_first & (s > 0) & (high < n_z))
        def _():
            take(high)

        @pl.when(low >= 0)
        def _():
            take(low)

        @pl.when(jnp.logical_not(up_first) & (s > 0) & (high < n_z))
        def _():
            take(high)

        return carry

    with jax.named_scope("rows"):
        lax.fori_loop(0, n_z, rows_step, 0)
    lane = lax.broadcasted_iota(jnp.int32, (n_tok, head_w), 1)

    def split_maps(ref, base):
        def one(h, carry):
            scaled = ref[:, pl.ds(pl.multiple_of(h * head_w, head_w), head_w)].astype(f32) * (
                (head_w // 2) ** -0.5
            )
            q_two[base + h, pl.ds(0, n_tok)] = jnp.where(lane < head_w // 2, scaled, 0.0).astype(bf16)
            q_two[base + h, pl.ds(n_tok, n_tok)] = jnp.where(lane < head_w // 2, 0.0, scaled).astype(bf16)
            return carry

        lax.fori_loop(0, per_head, one, 0)

    def attend(base, j, keys_at, n_keys, first, own, then=None):
        def one(h, carry):
            slot = base + h
            keys = k_all[j, pl.ds(keys_at, n_keys), pl.ds(pl.multiple_of(h * head_w, head_w), head_w)]
            values = v_all[j, pl.ds(keys_at, n_keys), pl.ds(pl.multiple_of(h * val_w, val_w), val_w)].T

            def score(m):
                scores = lax.dot_general(
                    keys,
                    q_two[slot, pl.ds(m * n_tok, n_tok)],
                    (((1,), (1,)), ((), ())),
                    preferred_element_type=f32,
                )
                if own:
                    scores = jnp.where(
                        lax.broadcasted_iota(jnp.int32, (n_keys, n_tok), 0)
                        <= lax.broadcasted_iota(jnp.int32, (n_keys, n_tok), 1),
                        scores,
                        neg_big,
                    )
                return scores

            both = [score(m) for m in range(2)]
            for m in range(2):
                part = pl.ds(m * n_tok, n_tok)
                scores = both[m]
                top = jnp.max(scores, axis=0, keepdims=True)
                if not first:
                    old = run_max[slot, :, part]
                    top = jnp.maximum(old, top)
                shares = jnp.exp(scores - top)
                total = jnp.sum(shares, axis=0, keepdims=True)
                update = dot(values, shares.astype(bf16))
                if not first:
                    shrink = jnp.exp(old - top)
                    total = total + run_sum[slot, :, part] * shrink
                    update = update + acc[slot, :, part] * shrink
                run_max[slot, :, part] = top
                run_sum[slot, :, part] = total
                acc[slot, :, part] = update
            if then is not None:
                then(h)
            return carry

        lax.fori_loop(0, per_head, one, 0)

    def attend_chip(base, j, first, then=None):
        with jax.named_scope("attend_chip"):
            attend(base, j, 0, lanes * n_tok, first, False, then)

    def core_at(core):
        return pl.multiple_of(core * n_tok, n_tok)

    with jax.named_scope("own"):
        split_maps(q_in, 0)
        attend(0, z, core_at(c), n_tok, True, True)
        kv_wait(z, 1 - c)

    @pl.when(c == 1)
    def _():
        attend(0, z, core_at(1 - c), n_tok, False, False)

    def kv_arrive(j):
        with jax.named_scope("kv_wait"):
            kv_wait(j, c)
        start_all(kv_copies_side(j))

    def put_lse(base, h):
        total = run_max[base + h] + jnp.log(run_sum[base + h])
        for m in range(2):
            lse_own[h, m : m + 1] = total[:, m * n_tok : (m + 1) * n_tok]
        lse_copy(h).start()

    def part_step(h):
        lse_copy(h).wait_recv()
        part_out[h] = mixed_maps(per_head, h, True).astype(bf16)
        part_copy(h).start()

    def mixed_maps(base, h, shared):
        maps = []
        for m in range(2):
            part = pl.ds(m * n_tok, n_tok)
            weight = 1.0 / run_sum[base + h, :, part]
            if shared:
                row = pl.ds(m, 1)
                weight = weight / (1.0 + jnp.exp(lse_far[h, row] - lse_own[h, row]))
            maps.append((acc[base + h, :, part], weight))
        (first, first_w), (second, second_w) = maps
        return first * first_w - second * (second_w * scale_ref[h])

    with jax.named_scope("w_wait"):
        for weight in weights:
            weight.wait()
    unit_rows = slots // 2
    n_rows = min(unit_rows, 64)
    tile_f = min(hidden_w, 256)

    def expert_in(unit):
        with jax.named_scope("arr_arrive"):
            tp_arrive(arr, arr_sems, 2, unit)

        def norm_step(i, carry):
            part = pl.ds(pl.multiple_of(unit * unit_rows + i * n_rows, n_rows), n_rows)
            squares = jnp.zeros((n_rows, 1), f32)
            for p in range(n_tp):
                x = arr[p, part].astype(f32)
                squares = squares + jnp.sum(x * x, axis=-1, keepdims=True)
            factor = lax.rsqrt(squares / (n_tp * cols) + eps)
            for p in range(n_tp):
                where = pl.ds(p * cols, cols)
                normed[part, where] = (
                    arr[p, part].astype(f32) * factor * norm_ref[0:1, where]
                ).astype(bf16)
            return carry

        with jax.named_scope("norm"):
            lax.fori_loop(0, unit_rows // n_rows, norm_step, 0)
        rows = pl.ds(unit * unit_rows, unit_rows)

        def gate_step(i, carry):
            where = pl.ds(pl.multiple_of(i * tile_f, tile_f), tile_f)
            gate = dot(normed[rows], wg[:, where])
            up = dot(normed[rows], wu[:, where])
            hid_all[t, rows, where] = (gate / (1.0 + jnp.exp(-gate)) * up).astype(bf16)
            return carry

        with jax.named_scope("gate"):
            lax.fori_loop(0, hidden_w // tile_f, gate_step, 0)

    def kv_wait_other(j):
        with jax.named_scope("kv_wait2"):
            kv_wait(j, 1 - c)

    expert_in(0)
    with jax.named_scope("arr_hand1"):
        tp_hand_on(arr, arr_sems, 2, 1)
    tp_send(hid_all, hid_sems, 2, 0)

    @pl.when(worker)
    def _():
        with jax.named_scope("q_wait"):
            q_copy.wait_recv()
        split_maps(q_far, per_head)
        attend_chip(per_head, z, True)

    def near_own():
        kv_wait_other(z - 1)
        attend_chip(0, z - 1, False, lambda h: put_lse(0, h))

    @pl.when(z == n_z - 2)
    def _():
        kv_arrive(z - 1)
        near_own()

    @pl.when(z != n_z - 2)
    def _():
        each_z(0, n_z, kv_got_from, kv_arrive)

    @pl.when(z == n_z - 1)
    def _():
        near_own()

    @pl.when(z < n_z - 2)
    def _():
        each_z(0, n_z, kv_got_from, kv_wait_other)

    @pl.when(worker)
    def _():
        each_z(0, z, kv_got_from, lambda j: attend_chip(per_head, j, False))

        for h in range(per_head):
            put_lse(per_head, h)

    @pl.when(worker & (z != n_z - 3))
    def _():
        for h in range(per_head):
            part_step(h)

    expert_in(1)
    with jax.named_scope("hid_hand0"):
        tp_hand_on(hid_all, hid_sems, 2, 0)
    tp_send(hid_all, hid_sems, 2, 1)

    @pl.when(z == n_z - 3)
    def _():
        for h in range(per_head):
            part_step(h)

    tile_o = min(out_w, 256)

    def expert_out(unit):
        with jax.named_scope("hid_arrive"):
            tp_arrive(hid_all, hid_sems, 2, unit)
        rows = pl.ds(unit * unit_rows, unit_rows)

        def down_step(i, carry):
            where = pl.ds(pl.multiple_of(i * tile_o, tile_o), tile_o)
            total = dot(hid_all[0, rows], wd[pl.ds(0, hidden_w), where])
            for p in range(1, n_tp):
                total = total + dot(hid_all[p, rows], wd[pl.ds(p * hidden_w, hidden_w), where])
            out_e[rows, where] = total.astype(bf16)
            return carry

        with jax.named_scope("down"):
            lax.fori_loop(0, out_w // tile_o, down_step, 0)
        ret_each(unit, lambda copy: copy.start())

    expert_out(0)

    @pl.when(z < n_z - 2)
    def _():
        each_z(0, z, kv_got_from, lambda j: attend_chip(0, j, False))

    with jax.named_scope("hid_hand1"):
        tp_hand_on(hid_all, hid_sems, 2, 1)
    expert_out(1)
    ret[pl.ds(pl.multiple_of(e * cap, cap), cap)] = out_e[pl.ds(first_slot(z, 0), cap)]

    gain = jnp.broadcast_to(gain_ref[...], (8, val_w)).T[:, 0:1]

    def head_step(h, mixed):
        mean_sq = jnp.mean(mixed * mixed, axis=0, keepdims=True)
        normal = mixed * lax.rsqrt(mean_sq + eps) * gain * head_factor
        head_all[t, :, h * val_w : (h + 1) * val_w] = normal.T.astype(bf16)
        tp_send(head_all, head_sems, per_head, h)

    @pl.when(z < n_z - 2)
    def _():
        for h in range(per_head):
            head_step(h, mixed_maps(0, h, False))

    @pl.when(upper)
    def _():
        for h in range(per_head):
            lse_copy(h).wait_recv()
            with jax.named_scope("part_wait"):
                part_copy(h).wait_recv()
            head_step(h, mixed_maps(0, h, True) + part_in[h].astype(f32))

    row_of = lax.broadcasted_iota(jnp.int32, (tok_b, tok_b), 0)
    col_of = lax.broadcasted_iota(jnp.int32, (tok_b, tok_b), 1)

    def column(row):
        return jnp.sum(
            jnp.where(row_of == col_of, row.astype(f32), 0.0), axis=1, keepdims=True
        )

    shares = []
    for k in range(route_count):
        ids = column(ids_ref[k : k + 1])
        same = jnp.zeros((tok_b, tok_b), f32)
        for other in range(route_count):
            same = same + (ids_ref[other : other + 1].astype(f32) == ids).astype(f32)
        ranks = jnp.sum(jnp.where(col_of < row_of, same, 0.0), axis=1, keepdims=True)
        slot = lax.broadcasted_iota(jnp.int32, (tok_b, slots), 1).astype(f32)
        spread[k] = jnp.where(slot == ids * cap + ranks, 1.0, 0.0).astype(bf16)
        shares.append(column(route_w_ref[k : k + 1]))

    with jax.named_scope("head_x"):
        for h in range(per_head):
            tp_hand_on(head_all, head_sems, per_head, h)
        for h in range(per_head):
            tp_arrive(head_all, head_sems, per_head, h)
    heads_w = head_all.shape[2]

    def mixer_step(i, carry):
        where = pl.ds(pl.multiple_of(i * tile_o, tile_o), tile_o)
        total = dot(head_all[0], wo[pl.ds(0, heads_w), where])
        for p in range(1, n_tp):
            total = total + dot(head_all[p], wo[pl.ds(p * heads_w, heads_w), where])
        mixer_ref[:, where] = total.astype(bf16)
        return carry

    with jax.named_scope("mixer"):
        lax.fori_loop(0, out_w // tile_o, mixer_step, 0)

    with jax.named_scope("ret_wait"):
        each_ep(lambda b: ret_arrival(b).wait_recv())
    tile_m = min(out_w, 256)
    for start in range(0, out_w, tile_m):
        where = pl.ds(start, tile_m)
        total = shares[0] * dot(spread[0], ret[:, where])
        for k in range(1, route_count):
            total = total + shares[k] * dot(spread[k], ret[:, where])
        mix_ref[:, where] = total.astype(bf16)

    with jax.named_scope("drain"):
        each_ep(lambda to: ids_copy(to).wait_send())
    for unit in range(2):
        ret_each(unit, lambda copy: copy.wait_send())
    tp_drain(arr, arr_sems, 2)
    tp_drain(hid_all, hid_sems, 2)
    tp_drain(head_all, head_sems, per_head)

    def drain(j, carry):
        rows_copy_side(j).wait_send()

        @pl.when((j >= z) & (z > 0) & (z < n_z - 2))
        def _():
            rows_copy_down(j).wait_send()

        @pl.when(kv_sent_to(j))
        def _():
            for copy in kv_copies_out(j):
                copy.wait_send()

        @pl.when((j == z) | kv_got_from(j))
        def _():
            for copy in kv_copies_side(j):
                copy.wait_send()

        return carry

    lax.fori_loop(0, n_z, drain, 0)

    @pl.when(upper)
    def _():
        q_copy.wait_send()

    @pl.when(upper | worker)
    def _():
        for h in range(per_head):
            lse_copy(h).wait_send()

    @pl.when(worker)
    def _():
        for h in range(per_head):
            part_copy(h).wait_send()


def per_device(
    n_ep,
    n_tp,
    query_rows,
    key_rows,
    value_rows,
    second_scale,
    head_gain,
    out_weight,
    routed_rows,
    norm_gain,
    route_ids,
    route_weight,
    expert_gate,
    expert_up,
    expert_down,
):
    n_tok, attn_w = query_rows.shape
    per_head = second_scale.shape[0]
    val_w = head_gain.shape[0]
    head_w = attn_w // per_head
    tok_b, cols = routed_rows.shape
    route_count = route_ids.shape[1]
    hidden_w = expert_gate.shape[2]
    out_w = out_weight.shape[1]
    n_z = n_ep // lanes
    cap = 2 * tok_b * route_count // n_ep
    slots = n_ep * cap
    vmem = pl.BlockSpec(memory_space=pltpu.VMEM)
    hbm = pl.BlockSpec(memory_space=pl.ANY)
    dma = pltpu.SemaphoreType.DMA
    return pl.pallas_call(
        functools.partial(layer_kernel, n_ep, n_tp),
        out_shape=(
            jax.ShapeDtypeStruct((n_tok, out_w), bf16),
            jax.ShapeDtypeStruct((tok_b, out_w), bf16),
        ),
        in_specs=[
            pl.BlockSpec(memory_space=pltpu.SMEM),
            hbm,
            hbm,
            hbm,
            vmem,
            hbm,
            hbm,
            vmem,
            vmem,
            vmem,
            hbm,
            hbm,
            hbm,
        ],
        out_specs=(vmem, vmem),
        scratch_shapes=[
            pltpu.VMEM((n_tok, attn_w), bf16),
            pltpu.VMEM((n_tok, attn_w), bf16),
            pltpu.VMEM((2 * per_head, 2 * n_tok, head_w), bf16),
            pltpu.VMEM((n_z, lanes * n_tok, attn_w), bf16),
            pltpu.VMEM((n_z, lanes * n_tok, value_rows.shape[1]), bf16),
            pltpu.VMEM((n_ep, tok_b, cols), bf16),
            pltpu.VMEM((n_ep, 8, tok_b), jnp.int32),
            pltpu.VMEM((n_tp, slots, cols), bf16),
            pltpu.VMEM((slots, n_tp * cols), bf16),
            pltpu.VMEM((n_tp, slots, hidden_w), bf16),
            pltpu.VMEM((slots, out_w), bf16),
            pltpu.VMEM((slots, out_w), bf16),
            pltpu.VMEM((n_tp, n_tok, per_head * val_w), bf16),
            pltpu.VMEM((route_count, tok_b, slots), bf16),
            pltpu.VMEM((2 * per_head, val_w, 2 * n_tok), f32),
            pltpu.VMEM((2 * per_head, 1, 2 * n_tok), f32),
            pltpu.VMEM((2 * per_head, 1, 2 * n_tok), f32),
            pltpu.VMEM((per_head, 2, n_tok), f32),
            pltpu.VMEM((per_head, 2, n_tok), f32),
            pltpu.VMEM((per_head, val_w, n_tok), bf16),
            pltpu.VMEM((per_head, val_w, n_tok), bf16),
            pltpu.VMEM(expert_gate.shape[1:], bf16),
            pltpu.VMEM(expert_up.shape[1:], bf16),
            pltpu.VMEM(expert_down.shape[1:], bf16),
            pltpu.VMEM(out_weight.shape, bf16),
            dma((4,)),
            dma((4,)),
            dma((n_z,)),
            dma((n_z,)),
            dma((n_z,)),
            dma((n_ep,)),
            dma((n_ep,)),
            dma((n_ep,)),
            dma((2, n_z)),
            dma((2, n_z)),
            dma((2, n_ep)),
            dma,
            dma,
            dma((per_head,)),
            dma((per_head,)),
            dma((per_head,)),
            dma((per_head,)),
            dma((n_tp, 4)),
            dma((n_tp, 4)),
            dma((n_tp, 4)),
            dma((n_tp, 4)),
            dma((n_tp, 2 * per_head)),
            dma((n_tp, 2 * per_head)),
            dma((n_ep,)),
            dma((n_ep,)),
        ],
        compiler_params=pltpu.CompilerParams(
            collective_id=0, has_side_effects=True, vmem_limit_bytes=66000000
        ),
    )(
        second_scale,
        query_rows,
        key_rows,
        value_rows,
        head_gain.reshape(1, -1),
        out_weight,
        routed_rows,
        norm_gain.reshape(1, -1),
        route_ids.T,
        route_weight.T,
        expert_gate,
        expert_up,
        expert_down,
    )


def solution(mesh):
    placed = (
        P("ep", "tp"),
        P("ep", "tp"),
        P("ep", "tp"),
        P("tp"),
        P(),
        P(None, "tp"),
        P("ep", "tp"),
        P(),
        P("ep", None),
        P("ep", None),
        P("ep", None, "tp"),
        P("ep", None, "tp"),
        P("ep", None, "tp"),
    )
    return jax.shard_map(
        functools.partial(per_device, mesh.shape["ep"], mesh.shape["tp"]),
        mesh=mesh,
        in_specs=placed,
        out_specs=(P("ep", "tp"), P("ep", "tp")),
        check_vma=False,
    )
```

```python
import functools

import jax
import jax.numpy as jnp
from jax import lax
from jax.experimental import pallas as pl
from jax.experimental.pallas import tpu as pltpu
from jax.sharding import PartitionSpec as P

eps = 1e-06
head_factor = 0.8
neg_big = -1e30
lanes = 2
f32 = jnp.float32
bf16 = jnp.bfloat16


def dot(a, b):
    return jnp.dot(a, b, preferred_element_type=f32)


def layer_kernel(
    n_ep,
    n_tp,
    scale_ref,
    q_hbm,
    k_hbm,
    v_hbm,
    gain_ref,
    wo_hbm,
    rows_hbm,
    norm_ref,
    ids_ref,
    route_w_ref,
    wg_hbm,
    wu_hbm,
    wd_hbm,
    mixer_ref,
    mix_ref,
    q_in,
    q_far,
    q_two,
    k_all,
    v_all,
    rows_all,
    ids_all,
    arr,
    normed,
    hid_all,
    out_e,
    ret,
    head_all,
    spread,
    acc,
    run_max,
    run_sum,
    lse_own,
    lse_far,
    part_out,
    part_in,
    wg,
    wu,
    wd,
    wo,
    local_sem,
    weight_sem,
    rows_up,
    rows_down,
    rows_side,
    rows_recv,
    ids_send,
    ids_recv,
    kv_out,
    kv_side,
    kv_recv,
    far_send,
    far_recv,
    lse_send,
    lse_recv,
    part_send,
    part_recv,
    arr_send,
    arr_recv,
    hid_send,
    hid_recv,
    head_send,
    head_recv,
    ret_send,
    ret_recv,
):
    e = lax.axis_index("ep")
    t = lax.axis_index("tp")
    n_z = n_ep // lanes
    z = lax.div(e, lanes)
    c = lax.rem(e, lanes)
    partner = z * lanes + (1 - c)
    n_tok = q_in.shape[0]
    tok_b = rows_all.shape[1]
    per_head = scale_ref.shape[0]
    head_w = q_two.shape[2]
    val_w = acc.shape[1]
    slots, out_w = ret.shape
    cap = slots // n_ep
    half = n_z // 2
    near = jnp.where(z < half, z, z - (half - 1))
    upper = z >= n_z - 2
    worker = (z >= n_z - 4) & (z < n_z - 2)
    far = jnp.where(upper, z - 2, lax.rem(z + 2, n_z)) * lanes + c
    cols = arr.shape[2]
    hidden_w = hid_all.shape[2]
    route_count = ids_ref.shape[0]

    def remote(src, dst, send, recv, ep_to, tp_to):
        return pltpu.make_async_remote_copy(
            src_ref=src,
            dst_ref=dst,
            send_sem=send,
            recv_sem=recv,
            device_id=(ep_to, tp_to),
            device_id_type=pl.DeviceIdType.MESH,
        )

    def kv_part(ref, j, core):
        return ref.at[j, pl.ds(pl.multiple_of(core * n_tok, n_tok), n_tok)]

    loads = [
        pltpu.make_async_copy(rows_hbm, rows_all.at[e], local_sem.at[0]),
        pltpu.make_async_copy(k_hbm, kv_part(k_all, z, c), local_sem.at[1]),
        pltpu.make_async_copy(v_hbm, kv_part(v_all, z, c), local_sem.at[2]),
        pltpu.make_async_copy(q_hbm, q_in, local_sem.at[3]),
    ]
    for load in loads:
        load.start()
    ids_all[e, pl.ds(0, route_count)] = ids_ref[...]
    weights = [
        pltpu.make_async_copy(wg_hbm.at[0], wg, weight_sem.at[0]),
        pltpu.make_async_copy(wu_hbm.at[0], wu, weight_sem.at[1]),
        pltpu.make_async_copy(wd_hbm.at[0], wd, weight_sem.at[2]),
        pltpu.make_async_copy(wo_hbm, wo, weight_sem.at[3]),
    ]

    barrier = pltpu.get_barrier_semaphore()

    def greet_ep(i, carry):
        to = lax.rem(e + i, n_ep)
        pl.semaphore_signal(barrier, inc=1, device_id=(to, t), device_id_type=pl.DeviceIdType.MESH)
        return carry

    def greet_tp(i, carry):
        to = lax.rem(t + i, n_tp)
        pl.semaphore_signal(barrier, inc=1, device_id=(e, to), device_id_type=pl.DeviceIdType.MESH)
        return carry

    lax.fori_loop(1, n_ep, greet_ep, 0)
    lax.fori_loop(1, n_tp, greet_tp, 0)
    with jax.named_scope("barrier"):
        pl.semaphore_wait(barrier, n_ep - 1 + n_tp - 1)
        for load in loads:
            load.wait()

    def ids_copy(to):
        return remote(ids_all.at[e], ids_all.at[e], ids_send.at[to], ids_recv.at[e], to, t)

    def ids_arrival(b):
        return remote(ids_all.at[b], ids_all.at[b], ids_send.at[b], ids_recv.at[b], b, t)

    def rows_copy(ref, block, send, recv, to):
        return remote(ref, ref, send, recv, to, t)

    def rows_part(j, k, sems, to):
        block = j * lanes + c
        ref = rows_all.at[block, pl.ds(k * (tok_b // 2), tok_b // 2)]
        return rows_copy(ref, block, sems.at[j, k], rows_recv.at[block, k], to)

    def rows_copy_up(j, k):
        return rows_part(j, k, rows_up, lax.rem(e + lanes, n_ep))

    def rows_copy_down(j, k):
        return rows_part(j, k, rows_down, lax.rem(e + n_ep - lanes, n_ep))

    def rows_copy_side(j, core):
        block = j * lanes + core
        return rows_copy(rows_all.at[block], block, rows_side.at[j], rows_recv.at[block, 0], partner)

    def kv_copies(j, core, sems, at, to):
        return [
            remote(
                kv_part(ref, j, core),
                kv_part(ref, j, core),
                sems.at[i, at],
                kv_recv.at[i, j * lanes + core],
                to,
                t,
            )
            for i, ref in enumerate((k_all, v_all))
        ]

    def kv_copies_out(j):
        return kv_copies(z, c, kv_out, j, j * lanes + c)

    def kv_copies_side(j):
        return kv_copies(j, c, kv_side, j, partner)

    def kv_sent_to(j):
        return (j > z) & ((j < n_z - 2) | (j == z + 1))

    def kv_got_from(j):
        return (j < z) & ((z < n_z - 2) | (j == z - 1))

    def kv_wait(j, core):
        for copy in kv_copies(j, core, kv_side, j, partner):
            copy.wait_recv()

    def each_z(first, last, cond, work):
        def one(j, carry):
            @pl.when(cond(j))
            def _():
                work(j)

            return carry

        lax.fori_loop(first, last, one, 0)

    def start_all(copies):
        for copy in copies:
            copy.start()

    q_copy = remote(q_in, q_far, far_send, far_recv, far, t)

    def lse_copy(h):
        return remote(lse_own.at[h], lse_far.at[h], lse_send.at[h], lse_recv.at[h], far, t)

    def part_copy(h):
        return remote(part_out.at[h], part_in.at[h], part_send.at[h], part_recv.at[h], far, t)

    square = n_tp == 4
    across = t + 1 - 2 * lax.rem(t, 2)
    along = lax.rem(t + 2, n_tp)
    corner = n_tp - 1 - t

    def piece(buf, source, i, units):
        if buf is head_all:
            step = n_tok // 2
            cols_at = pl.ds((i // 2) * val_w, val_w)
            return buf.at[source, pl.ds((i % 2) * step, step), cols_at]
        step = buf.shape[1] // (2 * units)
        return buf.at[source, pl.ds(i * step, step)]

    def tp_copy(buf, sems, units, source, i, row, to):
        ref = piece(buf, source, i, units)
        return remote(ref, ref, sems[0].at[row, i], sems[1].at[source, i], e, to)

    def tp_peers(work):
        def one(i, carry):
            to = lax.rem(t + i, n_tp)
            work(to, to)
            return carry

        if square:
            work(across, 0)
            work(along, 1)
        else:
            lax.fori_loop(1, n_tp, one, 0)

    def tp_send(buf, sems, units, unit):
        for i in (2 * unit, 2 * unit + 1):
            tp_peers(lambda to, row: tp_copy(buf, sems, units, t, i, row, to).start())

    def tp_hand_on(buf, sems, units, unit):
        if square:
            i = 2 * unit
            tp_copy(buf, sems, units, across, i, 2, across).wait_recv()
            tp_copy(buf, sems, units, across, i, 2, along).start()
            tp_copy(buf, sems, units, along, i + 1, 2, along).wait_recv()
            tp_copy(buf, sems, units, along, i + 1, 2, across).start()

    def tp_arrive(buf, sems, units, unit):
        i = 2 * unit
        if square:
            for source, at in ((across, i + 1), (along, i), (corner, i), (corner, i + 1)):
                tp_copy(buf, sems, units, source, at, 2, source).wait_recv()
        else:
            for at in (i, i + 1):
                tp_peers(lambda to, row: tp_copy(buf, sems, units, to, at, row, to).wait_recv())

    def tp_drain(buf, sems, units):
        for i in range(2 * units):
            tp_peers(lambda to, row: tp_copy(buf, sems, units, t, i, row, to).wait_send())
            if square:
                source, to = (across, along) if i % 2 == 0 else (along, across)
                tp_copy(buf, sems, units, source, i, 2, to).wait_send()

    arr_sems = (arr_send, arr_recv)
    hid_sems = (hid_send, hid_recv)
    head_sems = (head_send, head_recv)

    def unit_of(j):
        return jnp.where((j >= near) & (j < near + half), 0, 1)

    def first_slot(j, side):
        at = jnp.where(j < near, j, jnp.where(j < near + half, j - near, j - half))
        return pl.multiple_of(((unit_of(j) * 2 + side) * half + at) * cap, cap)

    def ret_part(b):
        return ret.at[pl.ds(pl.multiple_of(b * cap, cap), cap)]

    def ret_copy(j, side):
        to = j * lanes + (c if side == 0 else 1 - c)
        return remote(
            out_e.at[pl.ds(first_slot(j, side), cap)],
            ret_part(e),
            ret_send.at[to],
            ret_recv.at[e],
            to,
            t,
        )

    def ret_each(unit, work):
        def one(i, carry):
            j = near + i if unit == 0 else jnp.where(i < near, i, i + half)
            if unit == 0:

                @pl.when(j != z)
                def _():
                    work(ret_copy(j, 0))

            else:
                work(ret_copy(j, 0))
            work(ret_copy(j, 1))
            return carry

        lax.fori_loop(0, half, one, 0)

    def ret_arrival(b):
        return remote(ret_part(b), ret_part(b), ret_send.at[b], ret_recv.at[b], b, t)

    def each_ep(work):
        def one(i, carry):
            work(lax.rem(e + i, n_ep))
            return carry

        lax.fori_loop(1, n_ep, one, 0)

    each_ep(lambda to: ids_copy(to).start())

    def pick(block, j, side):
        ids = ids_all[block]
        hit = (ids[0:1] == e).astype(f32)
        for k in range(1, route_count):
            hit = hit + (ids[k : k + 1] == e).astype(f32)
        before = (
            lax.broadcasted_iota(jnp.int32, (tok_b, tok_b), 0)
            < lax.broadcasted_iota(jnp.int32, (tok_b, tok_b), 1)
        ).astype(bf16)
        ranks = dot(jnp.broadcast_to(hit, (16, tok_b)).astype(bf16), before)[0:1]
        slot = lax.broadcasted_iota(jnp.int32, (cap, tok_b), 0).astype(f32)
        chosen = jnp.where((slot == ranks) & (hit > 0.5), 1.0, 0.0).astype(bf16)
        start = first_slot(j, side)
        i = unit_of(j) * 2 + side
        arr[t, pl.ds(start, cap)] = dot(chosen, rows_all[block]).astype(bf16)
        part = arr.at[t, pl.ds(start, cap)]
        tp_peers(
            lambda to, row: remote(
                part, part, arr_send.at[row, i], arr_recv.at[t, i], e, to
            ).start()
        )

    def rows_left_up(j, carry):
        for k in range(2):
            rows_copy_up(j, k).wait_send()
        return carry

    def rows_left_down(j, carry):
        for k in range(2):
            rows_copy_down(j, k).wait_send()
        return carry

    def rows_step(s, carry):
        low, high = z - s, z + s

        for k in range(2):

            @pl.when((s > 0) & (low >= 0))
            def _():
                rows_copy_down(low, k).wait_recv()

            @pl.when((low >= 0) & (z + 1 < n_z))
            def _():
                rows_copy_up(low, k).start()

            @pl.when((s > 0) & (high < n_z))
            def _():
                rows_copy_up(high, k).wait_recv()

            @pl.when((high < n_z) & (z > 0))
            def _():
                rows_copy_down(high, k).start()

        @pl.when(s == 1)
        def _():
            start_all(kv_copies_side(z))
            for weight in weights:
                weight.start()

        @pl.when(s == z + 1)
        def _():
            lax.fori_loop(0, s, rows_left_up, 0)
            each_z(s, n_z, kv_sent_to, lambda j: start_all(kv_copies_out(j)))

        @pl.when(low >= 0)
        def _():
            rows_copy_side(low, c).start()

        @pl.when((s > 0) & (high < n_z))
        def _():
            rows_copy_side(high, c).start()

        @pl.when(s == half)
        def _():
            @pl.when(upper)
            def _():
                lax.fori_loop(z, n_z, rows_left_down, 0)
                q_copy.start()

            with jax.named_scope("arr_hand0"):
                tp_hand_on(arr, arr_sems, 2, 0)

        def take(j):
            mine, other = j * lanes + c, j * lanes + (1 - c)

            @pl.when(j != z)
            def _():
                ids_arrival(mine).wait_recv()

            pick(mine, j, 0)
            ids_arrival(other).wait_recv()
            rows_copy_side(j, 1 - c).wait_recv()
            pick(other, j, 1)

        up_first = z < half

        @pl.when(up_first & (s > 0) & (high < n_z))
        def _():
            take(high)

        @pl.when(low >= 0)
        def _():
            take(low)

        @pl.when(jnp.logical_not(up_first) & (s > 0) & (high < n_z))
        def _():
            take(high)

        return carry

    with jax.named_scope("rows"):
        lax.fori_loop(0, n_z, rows_step, 0)
    lane = lax.broadcasted_iota(jnp.int32, (n_tok, head_w), 1)

    def split_maps(ref, base):
        def one(h, carry):
            scaled = ref[:, pl.ds(pl.multiple_of(h * head_w, head_w), head_w)].astype(f32) * (
                (head_w // 2) ** -0.5
            )
            q_two[base + h, pl.ds(0, n_tok)] = jnp.where(lane < head_w // 2, scaled, 0.0).astype(bf16)
            q_two[base + h, pl.ds(n_tok, n_tok)] = jnp.where(lane < head_w // 2, 0.0, scaled).astype(bf16)
            return carry

        lax.fori_loop(0, per_head, one, 0)

    at_once = 2 - per_head % 2

    def attend(base, j, keys_at, n_keys, first, own, then=None):
        def score(h, m):
            scores = lax.dot_general(
                k_all[j, pl.ds(keys_at, n_keys), pl.ds(pl.multiple_of(h * head_w, head_w), head_w)],
                q_two[base + h, pl.ds(m * n_tok, n_tok)],
                (((1,), (1,)), ((), ())),
                preferred_element_type=f32,
            )
            if own:
                scores = jnp.where(
                    lax.broadcasted_iota(jnp.int32, (n_keys, n_tok), 0)
                    <= lax.broadcasted_iota(jnp.int32, (n_keys, n_tok), 1),
                    scores,
                    neg_big,
                )
            return scores

        def some(i, carry):
            group = [i * at_once + k for k in range(at_once)]
            every = [[score(h, m) for m in range(2)] for h in group]
            for h, both in zip(group, every):
                slot = base + h
                values = v_all[
                    j, pl.ds(keys_at, n_keys), pl.ds(pl.multiple_of(h * val_w, val_w), val_w)
                ].T
                for m in range(2):
                    part = pl.ds(m * n_tok, n_tok)
                    scores = both[m]
                    top = jnp.max(scores, axis=0, keepdims=True)
                    if not first:
                        old = run_max[slot, :, part]
                        top = jnp.maximum(old, top)
                    shares = jnp.exp(scores - top)
                    total = jnp.sum(shares, axis=0, keepdims=True)
                    update = dot(values, shares.astype(bf16))
                    if not first:
                        shrink = jnp.exp(old - top)
                        total = total + run_sum[slot, :, part] * shrink
                        update = update + acc[slot, :, part] * shrink
                    run_max[slot, :, part] = top
                    run_sum[slot, :, part] = total
                    acc[slot, :, part] = update
            if then is not None:
                for h in group:
                    then(h)
            return carry

        lax.fori_loop(0, per_head // at_once, some, 0)

    def attend_chip(base, j, first, then=None):
        with jax.named_scope("attend_chip"):
            attend(base, j, 0, lanes * n_tok, first, False, then)

    def core_at(core):
        return pl.multiple_of(core * n_tok, n_tok)

    with jax.named_scope("own"):
        split_maps(q_in, 0)
        attend(0, z, core_at(c), n_tok, True, True)
        kv_wait(z, 1 - c)

    inner = (z > 0) & (z < n_z - 1)

    @pl.when((c == 1) & inner)
    def _():
        attend(0, z, core_at(1 - c), n_tok, False, False)

    def kv_arrive(j):
        with jax.named_scope("kv_wait"):
            kv_wait(j, c)
        start_all(kv_copies_side(j))

    def put_lse(base, h):
        total = run_max[base + h] + jnp.log(run_sum[base + h])
        for m in range(2):
            lse_own[h, m : m + 1] = total[:, m * n_tok : (m + 1) * n_tok]
        lse_copy(h).start()

    def part_step(h):
        lse_copy(h).wait_recv()
        part_out[h] = mixed_maps(per_head, h, True).astype(bf16)
        part_copy(h).start()

    def mixed_maps(base, h, shared):
        maps = []
        for m in range(2):
            part = pl.ds(m * n_tok, n_tok)
            weight = 1.0 / run_sum[base + h, :, part]
            if shared:
                row = pl.ds(m, 1)
                weight = weight / (1.0 + jnp.exp(lse_far[h, row] - lse_own[h, row]))
            maps.append((acc[base + h, :, part], weight))
        (first, first_w), (second, second_w) = maps
        return first * first_w - second * (second_w * scale_ref[h])

    with jax.named_scope("w_wait"):
        for weight in weights:
            weight.wait()
    unit_rows = slots // 2
    n_rows = min(unit_rows, 64)
    tile_f = min(hidden_w, 256)

    def expert_in(unit):
        with jax.named_scope("arr_arrive"):
            tp_arrive(arr, arr_sems, 2, unit)

        def norm_step(i, carry):
            part = pl.ds(pl.multiple_of(unit * unit_rows + i * n_rows, n_rows), n_rows)
            squares = jnp.zeros((n_rows, 1), f32)
            for p in range(n_tp):
                x = arr[p, part].astype(f32)
                squares = squares + jnp.sum(x * x, axis=-1, keepdims=True)
            factor = lax.rsqrt(squares / (n_tp * cols) + eps)
            for p in range(n_tp):
                where = pl.ds(p * cols, cols)
                normed[part, where] = (
                    arr[p, part].astype(f32) * factor * norm_ref[0:1, where]
                ).astype(bf16)
            return carry

        with jax.named_scope("norm"):
            lax.fori_loop(0, unit_rows // n_rows, norm_step, 0)
        rows = pl.ds(unit * unit_rows, unit_rows)

        def gate_step(i, carry):
            where = pl.ds(pl.multiple_of(i * tile_f, tile_f), tile_f)
            gate = dot(normed[rows], wg[:, where])
            up = dot(normed[rows], wu[:, where])
            hid_all[t, rows, where] = (gate / (1.0 + jnp.exp(-gate)) * up).astype(bf16)
            return carry

        with jax.named_scope("gate"):
            lax.fori_loop(0, hidden_w // tile_f, gate_step, 0)

    def kv_wait_other(j):
        with jax.named_scope("kv_wait2"):
            kv_wait(j, 1 - c)

    expert_in(0)
    with jax.named_scope("arr_hand1"):
        tp_hand_on(arr, arr_sems, 2, 1)
    tp_send(hid_all, hid_sems, 2, 0)

    @pl.when((c == 1) & jnp.logical_not(inner))
    def _():
        attend(0, z, core_at(1 - c), n_tok, False, False)

    @pl.when(z != n_z - 2)
    def _():
        each_z(0, n_z, kv_got_from, kv_arrive)

    @pl.when(worker)
    def _():
        with jax.named_scope("q_wait"):
            q_copy.wait_recv()
        split_maps(q_far, per_head)
        attend_chip(per_head, z, True)

    def near_own():
        kv_wait_other(z - 1)
        attend_chip(0, z - 1, False, lambda h: put_lse(0, h))

    @pl.when(z == n_z - 2)
    def _():
        kv_arrive(z - 1)
        near_own()

    @pl.when(z == n_z - 1)
    def _():
        near_own()

    @pl.when(z < n_z - 2)
    def _():
        each_z(0, n_z, kv_got_from, kv_wait_other)

    @pl.when(worker)
    def _():
        each_z(0, z, kv_got_from, lambda j: attend_chip(per_head, j, False))

        for h in range(per_head):
            put_lse(per_head, h)

    @pl.when(worker & (z != n_z - 3))
    def _():
        for h in range(per_head):
            part_step(h)

    expert_in(1)
    with jax.named_scope("hid_hand0"):
        tp_hand_on(hid_all, hid_sems, 2, 0)
    tp_send(hid_all, hid_sems, 2, 1)

    @pl.when(z == n_z - 3)
    def _():
        for h in range(per_head):
            part_step(h)

    tile_o = min(out_w, 256)

    def expert_out(unit):
        with jax.named_scope("hid_arrive"):
            tp_arrive(hid_all, hid_sems, 2, unit)
        rows = pl.ds(unit * unit_rows, unit_rows)

        def down_step(i, carry):
            where = pl.ds(pl.multiple_of(i * tile_o, tile_o), tile_o)
            total = dot(hid_all[0, rows], wd[pl.ds(0, hidden_w), where])
            for p in range(1, n_tp):
                total = total + dot(hid_all[p, rows], wd[pl.ds(p * hidden_w, hidden_w), where])
            out_e[rows, where] = total.astype(bf16)
            return carry

        with jax.named_scope("down"):
            lax.fori_loop(0, out_w // tile_o, down_step, 0)
        ret_each(unit, lambda copy: copy.start())

    @pl.when(z < n_z - 2)
    def _():
        each_z(0, z, kv_got_from, lambda j: attend_chip(0, j, False))

    gain = jnp.broadcast_to(gain_ref[...], (8, val_w)).T[:, 0:1]

    def head_step(h, mixed):
        mean_sq = jnp.mean(mixed * mixed, axis=0, keepdims=True)
        normal = mixed * lax.rsqrt(mean_sq + eps) * gain * head_factor
        head_all[t, :, h * val_w : (h + 1) * val_w] = normal.T.astype(bf16)
        tp_send(head_all, head_sems, per_head, h)

    def heads(first, last):
        @pl.when(z < n_z - 2)
        def _():
            for h in range(first, last):
                head_step(h, mixed_maps(0, h, False))

        @pl.when(upper)
        def _():
            for h in range(first, last):
                lse_copy(h).wait_recv()
                with jax.named_scope("part_wait"):
                    part_copy(h).wait_recv()
                head_step(h, mixed_maps(0, h, True) + part_in[h].astype(f32))

    early = 0
    expert_out(0)

    @pl.when(z < n_z - 1)
    def _():
        heads(0, early)

    with jax.named_scope("hid_hand1"):
        tp_hand_on(hid_all, hid_sems, 2, 1)
    expert_out(1)

    @pl.when(z == n_z - 1)
    def _():
        heads(0, early)

    heads(early, per_head)

    ret[pl.ds(pl.multiple_of(e * cap, cap), cap)] = out_e[pl.ds(first_slot(z, 0), cap)]

    row_of = lax.broadcasted_iota(jnp.int32, (tok_b, tok_b), 0)
    col_of = lax.broadcasted_iota(jnp.int32, (tok_b, tok_b), 1)

    def column(row):
        return jnp.sum(
            jnp.where(row_of == col_of, row.astype(f32), 0.0), axis=1, keepdims=True
        )

    shares = []
    for k in range(route_count):
        ids = column(ids_ref[k : k + 1])
        same = jnp.zeros((tok_b, tok_b), f32)
        for other in range(route_count):
            same = same + (ids_ref[other : other + 1].astype(f32) == ids).astype(f32)
        ranks = jnp.sum(jnp.where(col_of < row_of, same, 0.0), axis=1, keepdims=True)
        slot = lax.broadcasted_iota(jnp.int32, (tok_b, slots), 1).astype(f32)
        spread[k] = jnp.where(slot == ids * cap + ranks, 1.0, 0.0).astype(bf16)
        shares.append(column(route_w_ref[k : k + 1]))

    with jax.named_scope("head_x"):
        for h in range(per_head):
            tp_hand_on(head_all, head_sems, per_head, h)

    with jax.named_scope("drain"):
        each_ep(lambda to: ids_copy(to).wait_send())
        tp_drain(arr, arr_sems, 2)
        tp_drain(hid_all, hid_sems, 2)

    def drain(j, carry):
        rows_copy_side(j, c).wait_send()

        @pl.when((j >= z) & (z > 0) & (z < n_z - 2))
        def _():
            for k in range(2):
                rows_copy_down(j, k).wait_send()

        @pl.when(kv_sent_to(j))
        def _():
            for copy in kv_copies_out(j):
                copy.wait_send()

        @pl.when((j == z) | kv_got_from(j))
        def _():
            for copy in kv_copies_side(j):
                copy.wait_send()

        return carry

    lax.fori_loop(0, n_z, drain, 0)

    @pl.when(upper)
    def _():
        q_copy.wait_send()

    @pl.when(upper | worker)
    def _():
        for h in range(per_head):
            lse_copy(h).wait_send()

    @pl.when(worker)
    def _():
        for h in range(per_head):
            part_copy(h).wait_send()

    with jax.named_scope("head_a"):
        for h in range(per_head):
            tp_arrive(head_all, head_sems, per_head, h)
    heads_w = head_all.shape[2]

    def mixer_step(i, carry):
        where = pl.ds(pl.multiple_of(i * tile_o, tile_o), tile_o)
        total = dot(head_all[0], wo[pl.ds(0, heads_w), where])
        for p in range(1, n_tp):
            total = total + dot(head_all[p], wo[pl.ds(p * heads_w, heads_w), where])
        mixer_ref[:, where] = total.astype(bf16)
        return carry

    with jax.named_scope("mixer"):
        lax.fori_loop(0, out_w // tile_o, mixer_step, 0)

    with jax.named_scope("ret_wait"):
        each_ep(lambda b: ret_arrival(b).wait_recv())
    tile_m = min(out_w, 256)
    for start in range(0, out_w, tile_m):
        where = pl.ds(start, tile_m)
        total = shares[0] * dot(spread[0], ret[:, where])
        for k in range(1, route_count):
            total = total + shares[k] * dot(spread[k], ret[:, where])
        mix_ref[:, where] = total.astype(bf16)

    for unit in range(2):
        ret_each(unit, lambda copy: copy.wait_send())
    tp_drain(head_all, head_sems, per_head)


def per_device(
    n_ep,
    n_tp,
    query_rows,
    key_rows,
    value_rows,
    second_scale,
    head_gain,
    out_weight,
    routed_rows,
    norm_gain,
    route_ids,
    route_weight,
    expert_gate,
    expert_up,
    expert_down,
):
    n_tok, attn_w = query_rows.shape
    per_head = second_scale.shape[0]
    val_w = head_gain.shape[0]
    head_w = attn_w // per_head
    tok_b, cols = routed_rows.shape
    route_count = route_ids.shape[1]
    hidden_w = expert_gate.shape[2]
    out_w = out_weight.shape[1]
    n_z = n_ep // lanes
    cap = 2 * tok_b * route_count // n_ep
    slots = n_ep * cap
    vmem = pl.BlockSpec(memory_space=pltpu.VMEM)
    hbm = pl.BlockSpec(memory_space=pl.ANY)
    dma = pltpu.SemaphoreType.DMA
    results = pl.pallas_call(
        functools.partial(layer_kernel, n_ep, n_tp),
        out_shape=(
            pltpu.VMEM((n_tok, out_w), bf16),
            pltpu.VMEM((tok_b, out_w), bf16),
        ),
        in_specs=[
            pl.BlockSpec(memory_space=pltpu.SMEM),
            hbm,
            hbm,
            hbm,
            vmem,
            hbm,
            hbm,
            vmem,
            vmem,
            vmem,
            hbm,
            hbm,
            hbm,
        ],
        out_specs=(vmem, vmem),
        scratch_shapes=[
            pltpu.VMEM((n_tok, attn_w), bf16),
            pltpu.VMEM((n_tok, attn_w), bf16),
            pltpu.VMEM((2 * per_head, 2 * n_tok, head_w), bf16),
            pltpu.VMEM((n_z, lanes * n_tok, attn_w), bf16),
            pltpu.VMEM((n_z, lanes * n_tok, value_rows.shape[1]), bf16),
            pltpu.VMEM((n_ep, tok_b, cols), bf16),
            pltpu.VMEM((n_ep, 8, tok_b), jnp.int32),
            pltpu.VMEM((n_tp, slots, cols), bf16),
            pltpu.VMEM((slots, n_tp * cols), bf16),
            pltpu.VMEM((n_tp, slots, hidden_w), bf16),
            pltpu.VMEM((slots, out_w), bf16),
            pltpu.VMEM((slots, out_w), bf16),
            pltpu.VMEM((n_tp, n_tok, per_head * val_w), bf16),
            pltpu.VMEM((route_count, tok_b, slots), bf16),
            pltpu.VMEM((2 * per_head, val_w, 2 * n_tok), f32),
            pltpu.VMEM((2 * per_head, 1, 2 * n_tok), f32),
            pltpu.VMEM((2 * per_head, 1, 2 * n_tok), f32),
            pltpu.VMEM((per_head, 2, n_tok), f32),
            pltpu.VMEM((per_head, 2, n_tok), f32),
            pltpu.VMEM((per_head, val_w, n_tok), bf16),
            pltpu.VMEM((per_head, val_w, n_tok), bf16),
            pltpu.VMEM(expert_gate.shape[1:], bf16),
            pltpu.VMEM(expert_up.shape[1:], bf16),
            pltpu.VMEM(expert_down.shape[1:], bf16),
            pltpu.VMEM(out_weight.shape, bf16),
            dma((4,)),
            dma((4,)),
            dma((n_z, 2)),
            dma((n_z, 2)),
            dma((n_z,)),
            dma((n_ep, 2)),
            dma((n_ep,)),
            dma((n_ep,)),
            dma((2, n_z)),
            dma((2, n_z)),
            dma((2, n_ep)),
            dma,
            dma,
            dma((per_head,)),
            dma((per_head,)),
            dma((per_head,)),
            dma((per_head,)),
            dma((n_tp, 4)),
            dma((n_tp, 4)),
            dma((n_tp, 4)),
            dma((n_tp, 4)),
            dma((n_tp, 2 * per_head)),
            dma((n_tp, 2 * per_head)),
            dma((n_ep,)),
            dma((n_ep,)),
        ],
        compiler_params=pltpu.CompilerParams(
            collective_id=0, has_side_effects=True, vmem_limit_bytes=65000000
        ),
    )(
        second_scale,
        query_rows,
        key_rows,
        value_rows,
        head_gain.reshape(1, -1),
        out_weight,
        routed_rows,
        norm_gain.reshape(1, -1),
        route_ids.T,
        route_weight.T,
        expert_gate,
        expert_up,
        expert_down,
    )
    return results


def solution(mesh):
    placed = (
        P("ep", "tp"),
        P("ep", "tp"),
        P("ep", "tp"),
        P("tp"),
        P(),
        P(None, "tp"),
        P("ep", "tp"),
        P(),
        P("ep", None),
        P("ep", None),
        P("ep", None, "tp"),
        P("ep", None, "tp"),
        P("ep", None, "tp"),
    )
    return jax.shard_map(
        functools.partial(per_device, mesh.shape["ep"], mesh.shape["tp"]),
        mesh=mesh,
        in_specs=placed,
        out_specs=(P("ep", "tp"), P("ep", "tp")),
        check_vma=False,
    )
```

```python
import functools

import jax
import jax.numpy as jnp
from jax import lax
from jax.experimental import pallas as pl
from jax.experimental.pallas import tpu as pltpu
from jax.sharding import PartitionSpec as P

eps = 1e-06
head_factor = 0.8
neg_big = -1e30
lanes = 2
f32 = jnp.float32
bf16 = jnp.bfloat16


def dot(a, b):
    return jnp.dot(a, b, preferred_element_type=f32)


def layer_kernel(
    n_ep,
    n_tp,
    scale_ref,
    q_hbm,
    k_hbm,
    v_hbm,
    gain_ref,
    wo_hbm,
    rows_hbm,
    norm_ref,
    ids_ref,
    route_w_ref,
    wg_hbm,
    wu_hbm,
    wd_hbm,
    mixer_ref,
    mix_ref,
    q_in,
    q_far,
    q_two,
    k_all,
    v_all,
    rows_all,
    ids_all,
    arr,
    normed,
    hid_all,
    out_e,
    ret,
    head_all,
    spread,
    mixer_sum,
    acc,
    run_max,
    run_sum,
    lse_own,
    lse_far,
    part_out,
    part_in,
    wg,
    wu,
    wd,
    wo,
    local_sem,
    weight_sem,
    rows_up,
    rows_down,
    rows_side,
    rows_recv,
    ids_send,
    ids_recv,
    kv_out,
    kv_side,
    kv_recv,
    far_send,
    far_recv,
    lse_send,
    lse_recv,
    part_send,
    part_recv,
    arr_send,
    arr_recv,
    hid_send,
    hid_recv,
    head_send,
    head_recv,
    ret_send,
    ret_recv,
):
    e = lax.axis_index("ep")
    t = lax.axis_index("tp")
    n_z = n_ep // lanes
    z = lax.div(e, lanes)
    c = lax.rem(e, lanes)
    partner = z * lanes + (1 - c)
    n_tok = q_in.shape[0]
    tok_b = rows_all.shape[1]
    per_head = scale_ref.shape[0]
    head_w = q_two.shape[2]
    val_w = acc.shape[1]
    slots, out_w = ret.shape
    cap = slots // n_ep
    half = n_z // 2
    near = jnp.where(z < half, z, z - (half - 1))
    upper = z >= n_z - 2
    worker = (z >= n_z - 4) & (z < n_z - 2)
    far = jnp.where(upper, z - 2, lax.rem(z + 2, n_z)) * lanes + c
    cols = arr.shape[2]
    hidden_w = hid_all.shape[2]
    route_count = ids_ref.shape[0]

    def remote(src, dst, send, recv, ep_to, tp_to):
        return pltpu.make_async_remote_copy(
            src_ref=src,
            dst_ref=dst,
            send_sem=send,
            recv_sem=recv,
            device_id=(ep_to, tp_to),
            device_id_type=pl.DeviceIdType.MESH,
        )

    def kv_part(ref, j, core):
        return ref.at[j, pl.ds(pl.multiple_of(core * n_tok, n_tok), n_tok)]

    loads = [
        pltpu.make_async_copy(rows_hbm, rows_all.at[e], local_sem.at[0]),
        pltpu.make_async_copy(k_hbm, kv_part(k_all, z, c), local_sem.at[1]),
        pltpu.make_async_copy(v_hbm, kv_part(v_all, z, c), local_sem.at[2]),
        pltpu.make_async_copy(q_hbm, q_in, local_sem.at[3]),
    ]
    for load in loads:
        load.start()
    ids_all[e, pl.ds(0, route_count)] = ids_ref[...]
    weights = [
        pltpu.make_async_copy(wg_hbm.at[0], wg, weight_sem.at[0]),
        pltpu.make_async_copy(wu_hbm.at[0], wu, weight_sem.at[1]),
        pltpu.make_async_copy(wd_hbm.at[0], wd, weight_sem.at[2]),
        pltpu.make_async_copy(wo_hbm, wo, weight_sem.at[3]),
    ]

    barrier = pltpu.get_barrier_semaphore()

    def greet_ep(i, carry):
        to = lax.rem(e + i, n_ep)
        pl.semaphore_signal(barrier, inc=1, device_id=(to, t), device_id_type=pl.DeviceIdType.MESH)
        return carry

    def greet_tp(i, carry):
        to = lax.rem(t + i, n_tp)
        pl.semaphore_signal(barrier, inc=1, device_id=(e, to), device_id_type=pl.DeviceIdType.MESH)
        return carry

    lax.fori_loop(1, n_ep, greet_ep, 0)
    lax.fori_loop(1, n_tp, greet_tp, 0)
    with jax.named_scope("barrier"):
        pl.semaphore_wait(barrier, n_ep - 1 + n_tp - 1)
        for load in loads:
            load.wait()

    def ids_copy(to):
        return remote(ids_all.at[e], ids_all.at[e], ids_send.at[to], ids_recv.at[e], to, t)

    def ids_arrival(b):
        return remote(ids_all.at[b], ids_all.at[b], ids_send.at[b], ids_recv.at[b], b, t)

    def rows_copy(ref, block, send, recv, to):
        return remote(ref, ref, send, recv, to, t)

    def rows_part(j, k, sems, to):
        block = j * lanes + c
        ref = rows_all.at[block, pl.ds(k * (tok_b // 2), tok_b // 2)]
        return rows_copy(ref, block, sems.at[j, k], rows_recv.at[block, k], to)

    def rows_copy_up(j, k):
        return rows_part(j, k, rows_up, lax.rem(e + lanes, n_ep))

    def rows_copy_down(j, k):
        return rows_part(j, k, rows_down, lax.rem(e + n_ep - lanes, n_ep))

    def rows_copy_side(j, core):
        block = j * lanes + core
        return rows_copy(rows_all.at[block], block, rows_side.at[j], rows_recv.at[block, 0], partner)

    def kv_copies(j, core, sems, at, to):
        return [
            remote(
                kv_part(ref, j, core),
                kv_part(ref, j, core),
                sems.at[i, at],
                kv_recv.at[i, j * lanes + core],
                to,
                t,
            )
            for i, ref in enumerate((k_all, v_all))
        ]

    def kv_copies_out(j):
        return kv_copies(z, c, kv_out, j, j * lanes + c)

    def kv_copies_side(j):
        return kv_copies(j, c, kv_side, j, partner)

    def kv_sent_to(j):
        return (j > z) & ((j < n_z - 2) | (j == z + 1))

    def kv_got_from(j):
        return (j < z) & ((z < n_z - 2) | (j == z - 1))

    def kv_wait(j, core):
        for copy in kv_copies(j, core, kv_side, j, partner):
            copy.wait_recv()

    def each_z(first, last, cond, work):
        def one(j, carry):
            @pl.when(cond(j))
            def _():
                work(j)

            return carry

        lax.fori_loop(first, last, one, 0)

    def start_all(copies):
        for copy in copies:
            copy.start()

    q_copy = remote(q_in, q_far, far_send, far_recv, far, t)

    def lse_copy(h):
        return remote(lse_own.at[h], lse_far.at[h], lse_send.at[h], lse_recv.at[h], far, t)

    def part_copy(h):
        return remote(part_out.at[h], part_in.at[h], part_send.at[h], part_recv.at[h], far, t)

    square = n_tp == 4
    across = t + 1 - 2 * lax.rem(t, 2)
    along = lax.rem(t + 2, n_tp)
    corner = n_tp - 1 - t

    def piece(buf, source, i, units):
        if buf is head_all:
            step = n_tok // 2
            cols_at = pl.ds((i // 2) * val_w, val_w)
            return buf.at[source, pl.ds((i % 2) * step, step), cols_at]
        step = buf.shape[1] // (2 * units)
        return buf.at[source, pl.ds(i * step, step)]

    def tp_copy(buf, sems, units, source, i, row, to):
        ref = piece(buf, source, i, units)
        return remote(ref, ref, sems[0].at[row, i], sems[1].at[source, i], e, to)

    def tp_peers(work):
        def one(i, carry):
            to = lax.rem(t + i, n_tp)
            work(to, to)
            return carry

        if square:
            work(across, 0)
            work(along, 1)
        else:
            lax.fori_loop(1, n_tp, one, 0)

    def tp_send(buf, sems, units, unit):
        for i in (2 * unit, 2 * unit + 1):
            tp_peers(lambda to, row: tp_copy(buf, sems, units, t, i, row, to).start())

    def tp_hand_on(buf, sems, units, unit):
        if square:
            i = 2 * unit
            tp_copy(buf, sems, units, across, i, 2, across).wait_recv()
            tp_copy(buf, sems, units, across, i, 2, along).start()
            tp_copy(buf, sems, units, along, i + 1, 2, along).wait_recv()
            tp_copy(buf, sems, units, along, i + 1, 2, across).start()

    def tp_arrive(buf, sems, units, unit):
        i = 2 * unit
        if square:
            for source, at in ((across, i + 1), (along, i), (corner, i), (corner, i + 1)):
                tp_copy(buf, sems, units, source, at, 2, source).wait_recv()
        else:
            for at in (i, i + 1):
                tp_peers(lambda to, row: tp_copy(buf, sems, units, to, at, row, to).wait_recv())

    def tp_drain(buf, sems, units):
        for i in range(2 * units):
            tp_peers(lambda to, row: tp_copy(buf, sems, units, t, i, row, to).wait_send())
            if square:
                source, to = (across, along) if i % 2 == 0 else (along, across)
                tp_copy(buf, sems, units, source, i, 2, to).wait_send()

    arr_sems = (arr_send, arr_recv)
    hid_sems = (hid_send, hid_recv)
    head_sems = (head_send, head_recv)

    def unit_of(j):
        return jnp.where((j >= near) & (j < near + half), 0, 1)

    def first_slot(j, side):
        at = jnp.where(j < near, j, jnp.where(j < near + half, j - near, j - half))
        return pl.multiple_of(((unit_of(j) * 2 + side) * half + at) * cap, cap)

    def ret_part(b):
        return ret.at[pl.ds(pl.multiple_of(b * cap, cap), cap)]

    def ret_copy(j, side):
        to = j * lanes + (c if side == 0 else 1 - c)
        return remote(
            out_e.at[pl.ds(first_slot(j, side), cap)],
            ret_part(e),
            ret_send.at[to],
            ret_recv.at[e],
            to,
            t,
        )

    def ret_each(unit, work):
        def one(i, carry):
            j = near + i if unit == 0 else jnp.where(i < near, i, i + half)
            if unit == 0:

                @pl.when(j != z)
                def _():
                    work(ret_copy(j, 0))

            else:
                work(ret_copy(j, 0))
            work(ret_copy(j, 1))
            return carry

        lax.fori_loop(0, half, one, 0)

    def ret_arrival(b):
        return remote(ret_part(b), ret_part(b), ret_send.at[b], ret_recv.at[b], b, t)

    def each_ep(work):
        def one(i, carry):
            work(lax.rem(e + i, n_ep))
            return carry

        lax.fori_loop(1, n_ep, one, 0)

    each_ep(lambda to: ids_copy(to).start())

    def pick(block, j, side):
        ids = ids_all[block]
        hit = (ids[0:1] == e).astype(f32)
        for k in range(1, route_count):
            hit = hit + (ids[k : k + 1] == e).astype(f32)
        before = (
            lax.broadcasted_iota(jnp.int32, (tok_b, tok_b), 0)
            < lax.broadcasted_iota(jnp.int32, (tok_b, tok_b), 1)
        ).astype(bf16)
        ranks = dot(jnp.broadcast_to(hit, (16, tok_b)).astype(bf16), before)[0:1]
        slot = lax.broadcasted_iota(jnp.int32, (cap, tok_b), 0).astype(f32)
        chosen = jnp.where((slot == ranks) & (hit > 0.5), 1.0, 0.0).astype(bf16)
        start = first_slot(j, side)
        i = unit_of(j) * 2 + side
        arr[t, pl.ds(start, cap)] = dot(chosen, rows_all[block]).astype(bf16)
        part = arr.at[t, pl.ds(start, cap)]
        tp_peers(
            lambda to, row: remote(
                part, part, arr_send.at[row, i], arr_recv.at[t, i], e, to
            ).start()
        )

    def rows_left_up(j, carry):
        for k in range(2):
            rows_copy_up(j, k).wait_send()
        return carry

    def rows_left_down(j, carry):
        for k in range(2):
            rows_copy_down(j, k).wait_send()
        return carry

    def rows_step(s, carry):
        low, high = z - s, z + s

        for k in range(2):

            @pl.when((s > 0) & (low >= 0))
            def _():
                rows_copy_down(low, k).wait_recv()

            @pl.when((low >= 0) & (z + 1 < n_z))
            def _():
                rows_copy_up(low, k).start()

            @pl.when((s > 0) & (high < n_z))
            def _():
                rows_copy_up(high, k).wait_recv()

            @pl.when((high < n_z) & (z > 0))
            def _():
                rows_copy_down(high, k).start()

        @pl.when(s == 1)
        def _():
            start_all(kv_copies_side(z))
            for weight in weights:
                weight.start()

        @pl.when(s == z + 1)
        def _():
            lax.fori_loop(0, s, rows_left_up, 0)
            each_z(s, n_z, kv_sent_to, lambda j: start_all(kv_copies_out(j)))

        @pl.when(low >= 0)
        def _():
            rows_copy_side(low, c).start()

        @pl.when((s > 0) & (high < n_z))
        def _():
            rows_copy_side(high, c).start()

        @pl.when(s == half)
        def _():
            @pl.when(upper)
            def _():
                lax.fori_loop(z, n_z, rows_left_down, 0)
                q_copy.start()

            with jax.named_scope("arr_hand0"):
                tp_hand_on(arr, arr_sems, 2, 0)

        def take(j):
            mine, other = j * lanes + c, j * lanes + (1 - c)

            @pl.when(j != z)
            def _():
                ids_arrival(mine).wait_recv()

            pick(mine, j, 0)
            ids_arrival(other).wait_recv()
            rows_copy_side(j, 1 - c).wait_recv()
            pick(other, j, 1)

        up_first = z < half

        @pl.when(up_first & (s > 0) & (high < n_z))
        def _():
            take(high)

        @pl.when(low >= 0)
        def _():
            take(low)

        @pl.when(jnp.logical_not(up_first) & (s > 0) & (high < n_z))
        def _():
            take(high)

        return carry

    with jax.named_scope("rows"):
        lax.fori_loop(0, n_z, rows_step, 0)
    lane = lax.broadcasted_iota(jnp.int32, (n_tok, head_w), 1)

    def split_maps(ref, base):
        def one(h, carry):
            scaled = ref[:, pl.ds(pl.multiple_of(h * head_w, head_w), head_w)].astype(f32) * (
                (head_w // 2) ** -0.5
            )
            q_two[base + h, pl.ds(0, n_tok)] = jnp.where(lane < head_w // 2, scaled, 0.0).astype(bf16)
            q_two[base + h, pl.ds(n_tok, n_tok)] = jnp.where(lane < head_w // 2, 0.0, scaled).astype(bf16)
            return carry

        lax.fori_loop(0, per_head, one, 0)

    at_once = 2 - per_head % 2

    def attend(base, j, keys_at, n_keys, first, own, then=None):
        def score(h, m):
            scores = lax.dot_general(
                k_all[j, pl.ds(keys_at, n_keys), pl.ds(pl.multiple_of(h * head_w, head_w), head_w)],
                q_two[base + h, pl.ds(m * n_tok, n_tok)],
                (((1,), (1,)), ((), ())),
                preferred_element_type=f32,
            )
            if own:
                scores = jnp.where(
                    lax.broadcasted_iota(jnp.int32, (n_keys, n_tok), 0)
                    <= lax.broadcasted_iota(jnp.int32, (n_keys, n_tok), 1),
                    scores,
                    neg_big,
                )
            return scores

        def some(i, carry):
            group = [i * at_once + k for k in range(at_once)]
            every = [[score(h, m) for m in range(2)] for h in group]
            for h, both in zip(group, every):
                slot = base + h
                values = v_all[
                    j, pl.ds(keys_at, n_keys), pl.ds(pl.multiple_of(h * val_w, val_w), val_w)
                ].T
                for m in range(2):
                    part = pl.ds(m * n_tok, n_tok)
                    scores = both[m]
                    top = jnp.max(scores, axis=0, keepdims=True)
                    if not first:
                        old = run_max[slot, :, part]
                        top = jnp.maximum(old, top)
                    shares = jnp.exp(scores - top)
                    total = jnp.sum(shares, axis=0, keepdims=True)
                    update = dot(values, shares.astype(bf16))
                    if not first:
                        shrink = jnp.exp(old - top)
                        total = total + run_sum[slot, :, part] * shrink
                        update = update + acc[slot, :, part] * shrink
                    run_max[slot, :, part] = top
                    run_sum[slot, :, part] = total
                    acc[slot, :, part] = update
            if then is not None:
                for h in group:
                    then(h)
            return carry

        lax.fori_loop(0, per_head // at_once, some, 0)

    def attend_chip(base, j, first, then=None):
        with jax.named_scope("attend_chip"):
            attend(base, j, 0, lanes * n_tok, first, False, then)

    def core_at(core):
        return pl.multiple_of(core * n_tok, n_tok)

    with jax.named_scope("own"):
        split_maps(q_in, 0)
        attend(0, z, core_at(c), n_tok, True, True)
        kv_wait(z, 1 - c)

    inner = (z > 0) & (z < n_z - 1)

    @pl.when((c == 1) & inner)
    def _():
        attend(0, z, core_at(1 - c), n_tok, False, False)

    def kv_arrive(j):
        with jax.named_scope("kv_wait"):
            kv_wait(j, c)
        start_all(kv_copies_side(j))

    def put_lse(base, h):
        total = run_max[base + h] + jnp.log(run_sum[base + h])
        for m in range(2):
            lse_own[h, m : m + 1] = total[:, m * n_tok : (m + 1) * n_tok]
        lse_copy(h).start()

    def part_step(h):
        lse_copy(h).wait_recv()
        part_out[h] = mixed_maps(per_head, h, True).astype(bf16)
        part_copy(h).start()

    def mixed_maps(base, h, shared):
        maps = []
        for m in range(2):
            part = pl.ds(m * n_tok, n_tok)
            weight = 1.0 / run_sum[base + h, :, part]
            if shared:
                row = pl.ds(m, 1)
                weight = weight / (1.0 + jnp.exp(lse_far[h, row] - lse_own[h, row]))
            maps.append((acc[base + h, :, part], weight))
        (first, first_w), (second, second_w) = maps
        return first * first_w - second * (second_w * scale_ref[h])

    with jax.named_scope("w_wait"):
        for weight in weights:
            weight.wait()
    unit_rows = slots // 2
    n_rows = min(unit_rows, 64)
    tile_f = min(hidden_w, 256)

    def expert_in(unit):
        with jax.named_scope("arr_arrive"):
            tp_arrive(arr, arr_sems, 2, unit)

        def norm_step(i, carry):
            part = pl.ds(pl.multiple_of(unit * unit_rows + i * n_rows, n_rows), n_rows)
            squares = jnp.zeros((n_rows, 1), f32)
            for p in range(n_tp):
                x = arr[p, part].astype(f32)
                squares = squares + jnp.sum(x * x, axis=-1, keepdims=True)
            factor = lax.rsqrt(squares / (n_tp * cols) + eps)
            for p in range(n_tp):
                where = pl.ds(p * cols, cols)
                normed[part, where] = (
                    arr[p, part].astype(f32) * factor * norm_ref[0:1, where]
                ).astype(bf16)
            return carry

        with jax.named_scope("norm"):
            lax.fori_loop(0, unit_rows // n_rows, norm_step, 0)
        rows = pl.ds(unit * unit_rows, unit_rows)

        def gate_step(i, carry):
            where = pl.ds(pl.multiple_of(i * tile_f, tile_f), tile_f)
            gate = dot(normed[rows], wg[:, where])
            up = dot(normed[rows], wu[:, where])
            hid_all[t, rows, where] = (gate / (1.0 + jnp.exp(-gate)) * up).astype(bf16)
            return carry

        with jax.named_scope("gate"):
            lax.fori_loop(0, hidden_w // tile_f, gate_step, 0)

    def kv_wait_other(j):
        with jax.named_scope("kv_wait2"):
            kv_wait(j, 1 - c)

    expert_in(0)

    @pl.when(z == n_z - 2)
    def _():
        kv_arrive(z - 1)

    with jax.named_scope("arr_hand1"):
        tp_hand_on(arr, arr_sems, 2, 1)
    tp_send(hid_all, hid_sems, 2, 0)

    @pl.when((c == 1) & jnp.logical_not(inner))
    def _():
        attend(0, z, core_at(1 - c), n_tok, False, False)

    @pl.when(z != n_z - 2)
    def _():
        each_z(0, n_z, kv_got_from, kv_arrive)

    @pl.when(worker)
    def _():
        with jax.named_scope("q_wait"):
            q_copy.wait_recv()
        split_maps(q_far, per_head)
        attend_chip(per_head, z, True)

    def near_own():
        kv_wait_other(z - 1)
        attend_chip(0, z - 1, False, lambda h: put_lse(0, h))

    @pl.when(z == n_z - 2)
    def _():
        near_own()

    @pl.when(z == n_z - 1)
    def _():
        near_own()

    @pl.when(z < n_z - 2)
    def _():
        each_z(0, n_z, kv_got_from, kv_wait_other)

    @pl.when(worker)
    def _():
        each_z(0, z, kv_got_from, lambda j: attend_chip(per_head, j, False))

        for h in range(per_head):
            put_lse(per_head, h)

    @pl.when(worker & (z != n_z - 3))
    def _():
        with jax.named_scope("part"):
            for h in range(per_head):
                part_step(h)

    expert_in(1)
    with jax.named_scope("hid_hand0"):
        tp_hand_on(hid_all, hid_sems, 2, 0)
    tp_send(hid_all, hid_sems, 2, 1)

    @pl.when(z == n_z - 3)
    def _():
        for h in range(per_head):
            part_step(h)

    tile_o = min(out_w, 256)

    def expert_out(unit):
        with jax.named_scope("hid_arrive"):
            tp_arrive(hid_all, hid_sems, 2, unit)
        rows = pl.ds(unit * unit_rows, unit_rows)

        def down_step(i, carry):
            where = pl.ds(pl.multiple_of(i * tile_o, tile_o), tile_o)
            total = dot(hid_all[0, rows], wd[pl.ds(0, hidden_w), where])
            for p in range(1, n_tp):
                total = total + dot(hid_all[p, rows], wd[pl.ds(p * hidden_w, hidden_w), where])
            out_e[rows, where] = total.astype(bf16)
            return carry

        with jax.named_scope("down"):
            lax.fori_loop(0, out_w // tile_o, down_step, 0)
        ret_each(unit, lambda copy: copy.start())

    @pl.when(z < n_z - 2)
    def _():
        each_z(0, z, kv_got_from, lambda j: attend_chip(0, j, False))

    gain = jnp.broadcast_to(gain_ref[...], (8, val_w)).T[:, 0:1]

    def head_step(h, mixed):
        mean_sq = jnp.mean(mixed * mixed, axis=0, keepdims=True)
        normal = mixed * lax.rsqrt(mean_sq + eps) * gain * head_factor
        head_all[t, :, h * val_w : (h + 1) * val_w] = normal.T.astype(bf16)
        tp_send(head_all, head_sems, per_head, h)

    def heads(first, last):
        @pl.when(z < n_z - 2)
        def _():
            for h in range(first, last):
                head_step(h, mixed_maps(0, h, False))

        @pl.when(upper)
        def _():
            for h in range(first, last):
                lse_copy(h).wait_recv()
                with jax.named_scope("part_wait"):
                    part_copy(h).wait_recv()
                head_step(h, mixed_maps(0, h, True) + part_in[h].astype(f32))

    expert_out(0)
    with jax.named_scope("hid_hand1"):
        tp_hand_on(hid_all, hid_sems, 2, 1)
    heads(0, per_head)
    expert_out(1)

    ret[pl.ds(pl.multiple_of(e * cap, cap), cap)] = out_e[pl.ds(first_slot(z, 0), cap)]

    row_of = lax.broadcasted_iota(jnp.int32, (tok_b, tok_b), 0)
    col_of = lax.broadcasted_iota(jnp.int32, (tok_b, tok_b), 1)

    def column(row):
        return jnp.sum(
            jnp.where(row_of == col_of, row.astype(f32), 0.0), axis=1, keepdims=True
        )

    shares = []
    for k in range(route_count):
        ids = column(ids_ref[k : k + 1])
        same = jnp.zeros((tok_b, tok_b), f32)
        for other in range(route_count):
            same = same + (ids_ref[other : other + 1].astype(f32) == ids).astype(f32)
        ranks = jnp.sum(jnp.where(col_of < row_of, same, 0.0), axis=1, keepdims=True)
        slot = lax.broadcasted_iota(jnp.int32, (tok_b, slots), 1).astype(f32)
        spread[k] = jnp.where(slot == ids * cap + ranks, 1.0, 0.0).astype(bf16)
        shares.append(column(route_w_ref[k : k + 1]))

    with jax.named_scope("head_x"):
        for h in range(per_head):
            tp_hand_on(head_all, head_sems, per_head, h)

    heads_w = head_all.shape[2]
    groups = per_head // at_once
    group_w = heads_w // groups

    def mixer_group(g):
        with jax.named_scope("head_a"):
            for h in range(g * at_once, (g + 1) * at_once):
                tp_arrive(head_all, head_sems, per_head, h)

        def step(i, carry):
            where = pl.ds(pl.multiple_of(i * tile_o, tile_o), tile_o)
            total = mixer_sum[:, where] if g > 0 else None
            for p in range(n_tp):
                more = dot(
                    head_all[p, :, g * group_w : (g + 1) * group_w],
                    wo[pl.ds(p * heads_w + g * group_w, group_w), where],
                )
                total = more if total is None else total + more
            if g < groups - 1:
                mixer_sum[:, where] = total
            else:
                mixer_ref[:, where] = total.astype(bf16)
            return carry

        with jax.named_scope("mixer"):
            lax.fori_loop(0, out_w // tile_o, step, 0)

    for g in range(groups - 1):
        mixer_group(g)

    with jax.named_scope("drain"):
        each_ep(lambda to: ids_copy(to).wait_send())
        tp_drain(arr, arr_sems, 2)
        tp_drain(hid_all, hid_sems, 2)

    def drain(j, carry):
        rows_copy_side(j, c).wait_send()

        @pl.when((j >= z) & (z > 0) & (z < n_z - 2))
        def _():
            for k in range(2):
                rows_copy_down(j, k).wait_send()

        @pl.when(kv_sent_to(j))
        def _():
            for copy in kv_copies_out(j):
                copy.wait_send()

        @pl.when((j == z) | kv_got_from(j))
        def _():
            for copy in kv_copies_side(j):
                copy.wait_send()

        return carry

    lax.fori_loop(0, n_z, drain, 0)

    @pl.when(upper)
    def _():
        q_copy.wait_send()

    @pl.when(upper | worker)
    def _():
        for h in range(per_head):
            lse_copy(h).wait_send()

    @pl.when(worker)
    def _():
        for h in range(per_head):
            part_copy(h).wait_send()

    mixer_group(groups - 1)

    with jax.named_scope("head_d"):
        ret_each(0, lambda copy: copy.wait_send())
        tp_drain(head_all, head_sems, per_head)
    with jax.named_scope("ret_wait"):
        each_ep(lambda b: ret_arrival(b).wait_recv())
    with jax.named_scope("mix"):
        tile_m = min(out_w, 256)
        for start in range(0, out_w, tile_m):
            where = pl.ds(start, tile_m)
            total = shares[0] * dot(spread[0], ret[:, where])
            for k in range(1, route_count):
                total = total + shares[k] * dot(spread[k], ret[:, where])
            mix_ref[:, where] = total.astype(bf16)

    ret_each(1, lambda copy: copy.wait_send())


def per_device(
    n_ep,
    n_tp,
    query_rows,
    key_rows,
    value_rows,
    second_scale,
    head_gain,
    out_weight,
    routed_rows,
    norm_gain,
    route_ids,
    route_weight,
    expert_gate,
    expert_up,
    expert_down,
):
    n_tok, attn_w = query_rows.shape
    per_head = second_scale.shape[0]
    val_w = head_gain.shape[0]
    head_w = attn_w // per_head
    tok_b, cols = routed_rows.shape
    route_count = route_ids.shape[1]
    hidden_w = expert_gate.shape[2]
    out_w = out_weight.shape[1]
    n_z = n_ep // lanes
    cap = 2 * tok_b * route_count // n_ep
    slots = n_ep * cap
    vmem = pl.BlockSpec(memory_space=pltpu.VMEM)
    hbm = pl.BlockSpec(memory_space=pl.ANY)
    dma = pltpu.SemaphoreType.DMA
    results = pl.pallas_call(
        functools.partial(layer_kernel, n_ep, n_tp),
        out_shape=(
            pltpu.VMEM((n_tok, out_w), bf16),
            pltpu.VMEM((tok_b, out_w), bf16),
        ),
        in_specs=[
            pl.BlockSpec(memory_space=pltpu.SMEM),
            hbm,
            hbm,
            hbm,
            vmem,
            hbm,
            hbm,
            vmem,
            vmem,
            vmem,
            hbm,
            hbm,
            hbm,
        ],
        out_specs=(vmem, vmem),
        scratch_shapes=[
            pltpu.VMEM((n_tok, attn_w), bf16),
            pltpu.VMEM((n_tok, attn_w), bf16),
            pltpu.VMEM((2 * per_head, 2 * n_tok, head_w), bf16),
            pltpu.VMEM((n_z, lanes * n_tok, attn_w), bf16),
            pltpu.VMEM((n_z, lanes * n_tok, value_rows.shape[1]), bf16),
            pltpu.VMEM((n_ep, tok_b, cols), bf16),
            pltpu.VMEM((n_ep, 8, tok_b), jnp.int32),
            pltpu.VMEM((n_tp, slots, cols), bf16),
            pltpu.VMEM((slots, n_tp * cols), bf16),
            pltpu.VMEM((n_tp, slots, hidden_w), bf16),
            pltpu.VMEM((slots, out_w), bf16),
            pltpu.VMEM((slots, out_w), bf16),
            pltpu.VMEM((n_tp, n_tok, per_head * val_w), bf16),
            pltpu.VMEM((route_count, tok_b, slots), bf16),
            pltpu.VMEM((n_tok, out_w), f32),
            pltpu.VMEM((2 * per_head, val_w, 2 * n_tok), f32),
            pltpu.VMEM((2 * per_head, 1, 2 * n_tok), f32),
            pltpu.VMEM((2 * per_head, 1, 2 * n_tok), f32),
            pltpu.VMEM((per_head, 2, n_tok), f32),
            pltpu.VMEM((per_head, 2, n_tok), f32),
            pltpu.VMEM((per_head, val_w, n_tok), bf16),
            pltpu.VMEM((per_head, val_w, n_tok), bf16),
            pltpu.VMEM(expert_gate.shape[1:], bf16),
            pltpu.VMEM(expert_up.shape[1:], bf16),
            pltpu.VMEM(expert_down.shape[1:], bf16),
            pltpu.VMEM(out_weight.shape, bf16),
            dma((4,)),
            dma((4,)),
            dma((n_z, 2)),
            dma((n_z, 2)),
            dma((n_z,)),
            dma((n_ep, 2)),
            dma((n_ep,)),
            dma((n_ep,)),
            dma((2, n_z)),
            dma((2, n_z)),
            dma((2, n_ep)),
            dma,
            dma,
            dma((per_head,)),
            dma((per_head,)),
            dma((per_head,)),
            dma((per_head,)),
            dma((n_tp, 4)),
            dma((n_tp, 4)),
            dma((n_tp, 4)),
            dma((n_tp, 4)),
            dma((n_tp, 2 * per_head)),
            dma((n_tp, 2 * per_head)),
            dma((n_ep,)),
            dma((n_ep,)),
        ],
        compiler_params=pltpu.CompilerParams(
            collective_id=0, has_side_effects=True, vmem_limit_bytes=65000000
        ),
    )(
        second_scale,
        query_rows,
        key_rows,
        value_rows,
        head_gain.reshape(1, -1),
        out_weight,
        routed_rows,
        norm_gain.reshape(1, -1),
        route_ids.T,
        route_weight.T,
        expert_gate,
        expert_up,
        expert_down,
    )
    return results


def solution(mesh):
    placed = (
        P("ep", "tp"),
        P("ep", "tp"),
        P("ep", "tp"),
        P("tp"),
        P(),
        P(None, "tp"),
        P("ep", "tp"),
        P(),
        P("ep", None),
        P("ep", None),
        P("ep", None, "tp"),
        P("ep", None, "tp"),
        P("ep", None, "tp"),
    )
    return jax.shard_map(
        functools.partial(per_device, mesh.shape["ep"], mesh.shape["tp"]),
        mesh=mesh,
        in_specs=placed,
        out_specs=(P("ep", "tp"), P("ep", "tp")),
        check_vma=False,
    )
```
